512 devices in a mesh: fs: 64 (over z, y), tp: 8 (over x, core).
Axes of the slice: x: 4, y: 8, z: 8, core: 2. Of those that a mesh axis runs over, the one named last changes fastest.
Arguments:
- tokens: bfloat16 [24576, 2048], P('fs', 'tp'), may hold values from -8 to 8
- w_value: bfloat16 [2048, 1024], P('fs', 'tp'), may hold values from -0.125 to 0.125
- w_gate: bfloat16 [2048, 1024], P('fs', 'tp'), may hold values from -0.125 to 0.125
- conv_kernel: bfloat16 [31, 1024], replicated, may hold values from -1 to 1
- conv_gain: float32 [1024], replicated, may hold values from 0.1 to 1.9
- w_mix_out: bfloat16 [1024, 2048], P('fs', 'tp'), may hold values from -0.1875 to 0.1875
- mix_gain: float32 [2048], replicated, may hold values from 0.1 to 1.9
- w_up: bfloat16 [2048, 8192], P('fs', 'tp'), may hold values from -0.125 to 0.125
- w_down: bfloat16 [8192, 2048], P('tp', 'fs'), may hold values from -0.0625 to 0.0625
- out_gain: float32 [2048], replicated, may hold values from 0.1 to 1.9
Outputs:
- result: bfloat16 [24576, 2048], P('fs', 'tp')
The draws below stay inside these ranges and needn't reach their ends.
All inputs are finite; a program needn't handle non-finite values.
Results may differ from the reference program's by a relative error of at most 0.013.
Values may be sent and summed in bfloat16 or wider, within the bound.
No kernel may reach another device: no remote copies, remote signals or barrier semaphores. Data moves between devices by JAX's collectives and lax.ppermute only.
A program may use at most 64 MiB of HBM per device.

```python
import math
import jax
import jax.numpy as jnp
from jax import lax

WIDTH = 2048
CHANNELS = 1024
UNITS = 8192
KERNEL = 31
LENGTH = 128
TOK_DEV = 384
TOKENS = 24576
N_FS = 64
N_TP = 8


def draw_tokens(key, part):
    scale_key, value_key, shift_key = jax.random.split(jax.random.fold_in(key, 11), 3)
    block_scales = jnp.exp(jax.random.uniform(scale_key, (8,), jnp.float32, math.log(0.3), math.log(3.0)))
    column_scales = jnp.repeat(block_scales, WIDTH // 8)
    raw = jax.random.normal(value_key, (TOKENS, WIDTH), jnp.float32)
    return jnp.clip(raw * column_scales, -8.0, 8.0).astype(jnp.bfloat16)


def block_levels(key, dims, pieces, low, top_value):
    gain, own = 1.0, jax.random.fold_in(key, 6)
    for axis_at, blocks in pieces:
        steps = jnp.exp(jax.random.uniform(jax.random.fold_in(own, axis_at), (blocks,), jnp.float32, low / len(pieces), top_value / len(pieces)))
        gain = gain * jnp.repeat(steps, dims[axis_at] // blocks).reshape([-1 if axis == axis_at else 1 for axis in range(len(dims))])
    return gain


def bell_draw(stream_key, dims, deviation, bound, pieces=(), held_as=jnp.bfloat16):
    result = deviation * jax.random.normal(stream_key, dims, jnp.float32)
    if pieces:
        result = result * block_levels(stream_key, dims, pieces, -0.22, 0.18)
    return jnp.clip(result, -bound, bound).astype(held_as)


def setup_inputs(seed: int = 0) -> dict:
    streams_of = jax.random.split(jax.random.key(seed), 11)
    tokens = draw_tokens(jax.random.fold_in(streams_of[10], 71), 0)
    w_value = bell_draw(streams_of[1], (WIDTH, CHANNELS), WIDTH ** -0.5, 0.125, ((0, 64), (1, 8)))
    w_gate = bell_draw(streams_of[2], (WIDTH, CHANNELS), WIDTH ** -0.5, 0.125, ((0, 64), (1, 8)))
    conv_kernel = bell_draw(streams_of[3], (KERNEL, CHANNELS), KERNEL ** -0.5, 1.0)
    conv_gain = jnp.clip(1.0 + 0.18 * jax.random.normal(streams_of[4], (CHANNELS,), jnp.float32), 0.1, 1.9)
    w_mix_out = bell_draw(streams_of[5], (CHANNELS, WIDTH), CHANNELS ** -0.5, 0.1875, ((0, 64), (1, 8)))
    mix_gain = jnp.clip(1.0 + 0.18 * jax.random.normal(streams_of[6], (WIDTH,), jnp.float32), 0.1, 1.9)
    w_up = bell_draw(streams_of[7], (WIDTH, UNITS), WIDTH ** -0.5, 0.125, ((0, 64), (1, 8)))
    w_down = bell_draw(streams_of[8], (UNITS, WIDTH), UNITS ** -0.5, 0.0625, ((0, 8), (1, 64)))
    out_gain = jnp.clip(1.0 + 0.18 * jax.random.normal(streams_of[9], (WIDTH,), jnp.float32), 0.1, 1.9)
    return {"tokens": tokens, "w_value": w_value, "w_gate": w_gate, "conv_kernel": conv_kernel, "conv_gain": conv_gain, "w_mix_out": w_mix_out, "mix_gain": mix_gain, "w_up": w_up, "w_down": w_down, "out_gain": out_gain}


norm_eps = 1e-05
residual_scale = 2.0 ** 0.5

def causal_filter(gated, kernel):
    sequences = gated.shape[0] // LENGTH
    frames = gated.astype(jnp.float32).reshape(sequences, LENGTH, gated.shape[1])
    padded = jnp.pad(frames, ((0, 0), (KERNEL - 1, 0), (0, 0)))
    accumulated = jnp.zeros(frames.shape, jnp.float32)
    for offset in range(KERNEL):
        accumulated = accumulated + kernel[offset].astype(jnp.float32) * padded[:, offset:offset + LENGTH]
    return accumulated.reshape(gated.shape[0], gated.shape[1])

def normalize(values, total_sum, total_sq, entries, gain_vector):
    average = total_sum / entries
    spread = jnp.maximum(total_sq / entries - average * average, 0.0)
    return (values - average[:, None]) * lax.rsqrt(spread[:, None] + norm_eps) * gain_vector.astype(jnp.float32)

def reference(tokens, w_value, w_gate, conv_kernel, conv_gain, w_mix_out, mix_gain, w_up, w_down, out_gain):

    def one_block(frames):
        values_proj = jnp.dot(frames, w_value, preferred_element_type=jnp.float32)
        gate_proj = jnp.dot(frames, w_gate, preferred_element_type=jnp.float32)
        gated = (values_proj * jax.nn.sigmoid(gate_proj)).astype(jnp.bfloat16)
        filtered = causal_filter(gated, conv_kernel)
        normed = normalize(filtered, lax.optimization_barrier(jnp.sum(filtered, 1)), lax.optimization_barrier(jnp.sum(filtered * filtered, 1)), CHANNELS, conv_gain)
        activated = jax.nn.silu(normed).astype(jnp.bfloat16)
        mixed = jnp.dot(activated, w_mix_out, preferred_element_type=jnp.float32)
        combined = residual_scale * frames.astype(jnp.float32) + mixed
        middle = normalize(combined, lax.optimization_barrier(jnp.sum(combined, 1)), lax.optimization_barrier(jnp.sum(combined * combined, 1)), WIDTH, mix_gain).astype(jnp.bfloat16)
        up_proj = jnp.dot(middle, w_up, preferred_element_type=jnp.float32)
        hidden = jnp.square(jax.nn.relu(up_proj)).astype(jnp.bfloat16)
        share_size = UNITS // N_TP
        down_sum = jnp.zeros((frames.shape[0], WIDTH), jnp.float32)
        for block_index in range(N_TP):
            lower = block_index * share_size
            piece_sum = jnp.dot(hidden[:, lower:lower + share_size], w_down[lower:lower + share_size], preferred_element_type=jnp.float32).astype(jnp.bfloat16)
            piece_sum = lax.optimization_barrier(piece_sum)
            down_sum = down_sum + piece_sum.astype(jnp.float32)
        final = residual_scale * middle.astype(jnp.float32) + down_sum
        return normalize(final, lax.optimization_barrier(jnp.sum(final, 1)), lax.optimization_barrier(jnp.sum(final * final, 1)), WIDTH, out_gain).astype(jnp.bfloat16)
    blocks = tokens.reshape(N_FS, TOK_DEV, WIDTH)
    return lax.map(one_block, blocks).reshape(TOKENS, WIDTH)
```

```python
import jax
import jax.numpy as jnp
from jax import lax
from jax.sharding import Mesh
from jax.sharding import PartitionSpec as P

WIDTH = 2048
CHANNELS = 1024
KERNEL = 31
LENGTH = 128
FS = ("z", "y")
TP = ("x", "core")


norm_eps = 1e-05
residual_scale = 2.0**0.5


def sent_to_all(shard, axis):
    copies = jnp.broadcast_to(shard, (lax.axis_size(axis), *shard.shape))
    return lax.all_to_all(copies, axis, split_axis=0, concat_axis=0, tiled=True)


def joined_columns(parts):
    return jnp.moveaxis(parts, 0, 1).reshape(parts.shape[1], -1)


def shifted(a, axis, by):
    n = lax.axis_size(axis)
    return lax.ppermute(a, axis, [(i, (i + by) % n) for i in range(n)])


def ring_pieces(piece, axis):
    half = piece.shape[0] // 2
    from_below, from_above = [piece], [piece]
    for _ in range(3):
        from_below.append(shifted(from_below[-1], axis, 1))
        from_above.append(shifted(from_above[-1], axis, -1))
    far_low = shifted(from_below[3][:half], axis, 1)
    far_high = shifted(from_above[3][half:], axis, -1)
    far = [far_low, far_high]
    return [[piece], [from_above[1]], [from_above[2]], [from_above[3]], far, [from_below[3]], [from_below[2]], [from_below[1]]]


def causal_filter(gated, kernel):
    sequences = gated.shape[0] // LENGTH
    frames = gated.astype(jnp.float32).reshape(sequences, LENGTH, gated.shape[1])
    padded = jnp.pad(frames, ((0, 0), (KERNEL - 1, 0), (0, 0)))
    accumulated = jnp.zeros(frames.shape, jnp.float32)
    for offset in range(KERNEL):
        accumulated = (
            accumulated + kernel[offset].astype(jnp.float32) * padded[:, offset : offset + LENGTH]
        )
    return accumulated.reshape(gated.shape[0], gated.shape[1])


def row_norm_terms(values, entries):
    average = jnp.sum(values, 1, keepdims=True) / entries
    spread = jnp.maximum(jnp.sum(values * values, 1, keepdims=True) / entries - average * average, 0.0)
    return average, lax.rsqrt(spread + norm_eps)


def per_device(
    tokens, w_value, w_gate, conv_kernel, conv_gain, w_mix_out, mix_gain, w_up, w_down, out_gain
):
    tp_rank = lax.axis_index(TP)
    y_rank = lax.axis_index("y")
    width_part = tokens.shape[1]
    channel_part = w_value.shape[1]
    f32 = jnp.float32
    up_whole = lax.all_gather(w_up, FS, axis=0, tiled=True)

    value_z = sent_to_all(w_value, "z")
    gate_y = sent_to_all(w_gate, "y")
    value_whole = sent_to_all(value_z, "y").transpose(1, 0, 2, 3).reshape(WIDTH, channel_part)
    gate_whole = sent_to_all(gate_y, "z").reshape(WIDTH, channel_part)

    features = joined_columns(sent_to_all(tokens, TP))

    mix_z = sent_to_all(w_mix_out, "z")
    mix_whole = sent_to_all(mix_z, "y").transpose(1, 0, 2, 3).reshape(CHANNELS, width_part)

    down_z = sent_to_all(w_down.T, "z")
    down_pieces = ring_pieces(down_z.reshape(-1, down_z.shape[-1]), "y")

    values_proj = jnp.dot(features, value_whole, preferred_element_type=f32)
    gate_proj = jnp.dot(features, gate_whole, preferred_element_type=f32)
    gated = (values_proj * jax.nn.sigmoid(gate_proj)).astype(jnp.bfloat16)
    kernel = lax.dynamic_slice_in_dim(conv_kernel, tp_rank * channel_part, channel_part, 1)
    filtered = causal_filter(gated, kernel)
    filtered_whole = joined_columns(sent_to_all(filtered.astype(jnp.bfloat16), TP)).astype(f32)
    average, scale = row_norm_terms(filtered_whole, CHANNELS)
    activated = jax.nn.silu((filtered_whole - average) * scale * conv_gain).astype(jnp.bfloat16)

    mixed = jnp.dot(activated, mix_whole, preferred_element_type=f32)
    combined = residual_scale * tokens.astype(f32) + mixed
    combined_whole = joined_columns(sent_to_all(combined.astype(jnp.bfloat16), TP)).astype(f32)
    average, scale = row_norm_terms(combined_whole, WIDTH)
    middle_whole = ((combined_whole - average) * scale * mix_gain).astype(jnp.bfloat16)
    middle_gain = lax.dynamic_slice_in_dim(mix_gain, tp_rank * width_part, width_part, 0)
    middle = ((combined - average) * scale * middle_gain).astype(jnp.bfloat16)

    up_proj = jnp.dot(middle_whole, up_whole, preferred_element_type=f32)
    hidden = jnp.square(jax.nn.relu(up_proj)).astype(jnp.bfloat16)

    def rows_out(piece):
        return lax.dot_general(
            piece, hidden, (((1,), (1,)), ((), ())), preferred_element_type=f32
        ).astype(jnp.bfloat16)

    terms = []
    for parts in down_pieces:
        outs = [rows_out(p) for p in parts]
        terms.append(outs[0] if len(outs) == 1 else jnp.concatenate(outs, 0))
    ranks = lax.axis_size(TP)
    near = lax.axis_size("y")
    sent = jnp.stack([t.reshape(ranks, -1, t.shape[-1]) for t in terms], 1)
    arrived = lax.all_to_all(sent, TP, 0, 0, tiled=True)
    down_sum = jnp.sum(arrived.astype(f32), 0)
    down_sum = jnp.roll(down_sum, y_rank, 0).reshape(width_part, -1).T

    final = residual_scale * middle.astype(f32) + down_sum
    sums = jnp.stack([jnp.sum(final, 1), jnp.sum(final * final, 1)])
    totals = jnp.sum(sent_to_all(sums, TP), 0)
    average = totals[0] / WIDTH
    spread = jnp.maximum(totals[1] / WIDTH - average * average, 0.0)
    final_gain = lax.dynamic_slice_in_dim(out_gain, tp_rank * width_part, width_part, 0)
    result = (final - average[:, None]) * lax.rsqrt(spread[:, None] + norm_eps) * final_gain
    return result.astype(jnp.bfloat16)


def solution(mesh):
    split = Mesh(mesh.devices.reshape(8, 8, 4, 2), ("z", "y", "x", "core"))
    in_specs = (
        P(FS, TP),
        P(FS, TP),
        P(FS, TP),
        P(),
        P(),
        P(FS, TP),
        P(),
        P(FS, TP),
        P(TP, FS),
        P(),
    )
    return jax.shard_map(
        per_device, mesh=split, in_specs=in_specs, out_specs=P(FS, TP), check_vma=False
    )
```

```python
import jax
import jax.numpy as jnp
import numpy as np
from jax import lax
from jax.sharding import Mesh
from jax.sharding import PartitionSpec as P


WIDTH = 2048
CHANNELS = 1024
KERNEL = 31
LENGTH = 128
FS = ("z", "y")
TP = ("x", "core")
ALL = ("z", "y", "x", "core")
SIDE = 8


norm_eps = 1e-05
residual_scale = 2.0**0.5
f32 = jnp.float32
bf16 = jnp.bfloat16


def rings(axis_of_core):
    ids = np.arange(SIDE * SIDE * 4 * 2).reshape(SIDE, SIDE, 4, 2)
    out = []
    for x in range(4):
        for core in range(2):
            plane = ids[:, :, x, core]
            out += (plane if axis_of_core[core] == "y" else plane.T).tolist()
    return out


FIRST, SECOND = rings("yz"), rings("zy")


def sent_to_group(shard, groups):
    copies = jnp.broadcast_to(shard, (SIDE, *shard.shape))
    return lax.all_to_all(copies, ALL, 0, 0, axis_index_groups=groups, tiled=True)


def partner_of(a):
    return lax.ppermute(a, "core", [(0, 1), (1, 0)])


def turned(core, a):
    return jnp.where(core == 0, a, jnp.swapaxes(a, 0, 1))


def all_ranks(shard, core):
    copies = jnp.broadcast_to(shard, (4, *shard.shape))
    mine = lax.all_to_all(copies, "x", 0, 0, tiled=True)
    other = partner_of(mine)
    both = jnp.stack([jnp.where(core == 0, mine, other), jnp.where(core == 0, other, mine)], 1)
    return both.reshape(SIDE, *shard.shape)


def joined_columns(parts):
    return jnp.moveaxis(parts, 0, 1).reshape(parts.shape[1], -1)


def causal_filter(gated, kernel):
    sequences = gated.shape[0] // LENGTH
    frames = gated.astype(f32).reshape(sequences, LENGTH, gated.shape[1])
    padded = jnp.pad(frames, ((0, 0), (KERNEL - 1, 0), (0, 0)))
    accumulated = jnp.zeros(frames.shape, f32)
    for offset in range(KERNEL):
        accumulated = (
            accumulated + kernel[offset].astype(f32) * padded[:, offset : offset + LENGTH]
        )
    return accumulated.reshape(gated.shape[0], gated.shape[1])


def row_norm_terms(values, entries):
    average = jnp.sum(values, 1, keepdims=True) / entries
    spread = jnp.maximum(jnp.sum(values * values, 1, keepdims=True) / entries - average * average, 0.0)
    return average, lax.rsqrt(spread + norm_eps)


def layer(
    tokens, w_value, w_gate, conv_kernel, conv_gain, w_mix_out, mix_gain, w_up, w_down, out_gain
):
    tp_rank = lax.axis_index(TP)
    core = lax.axis_index("core")
    frames = tokens.shape[0]
    width_part = tokens.shape[1]
    channel_part = w_value.shape[1]
    units_part = w_up.shape[1]

    def mine_of(vector, size):
        return lax.dynamic_slice_in_dim(vector, tp_rank * size, size, vector.ndim - 1)

    wide = jnp.concatenate([w_up, w_down.T], 1)
    wide = lax.all_gather(wide, ALL, axis=0, tiled=True, axis_index_groups=FIRST)
    wide = lax.all_gather(wide, ALL, axis=0, tiled=True, axis_index_groups=SECOND)

    mix_rows = w_mix_out.shape[0]
    halves = [w_mix_out[:, :channel_part], w_mix_out[:, channel_part:]]
    small = jnp.concatenate([w_value, w_gate, jnp.concatenate(halves, 0)], 1)
    small = sent_to_group(small, FIRST).reshape(-1, small.shape[1])
    small = sent_to_group(small, SECOND)
    value_gate = small[:, :, : 2 * channel_part].reshape(WIDTH, 2 * channel_part)
    mix = small[:, :, 2 * channel_part :].reshape(SIDE, SIDE, 2, mix_rows, channel_part)
    mix = turned(core, mix.transpose(0, 1, 3, 2, 4)).reshape(CHANNELS, width_part)

    ranks = all_ranks(tokens.T, core)
    ranks = turned(core, ranks.reshape(SIDE, SIDE, -1, frames)).reshape(WIDTH, frames)

    both = lax.dot_general(ranks, value_gate, (((0,), (0,)), ((), ())), preferred_element_type=f32)
    values_proj, gate_proj = both[:, :channel_part], both[:, channel_part:]
    gated = (values_proj * jax.nn.sigmoid(gate_proj)).astype(bf16)
    filtered = causal_filter(gated, mine_of(conv_kernel, channel_part))
    filtered_whole = joined_columns(all_ranks(filtered.astype(bf16), core)).astype(f32)
    average, scale = row_norm_terms(filtered_whole, CHANNELS)
    activated = jax.nn.silu((filtered_whole - average) * scale * conv_gain).astype(bf16)

    mixed = jnp.dot(activated, mix, preferred_element_type=f32)
    combined = residual_scale * tokens.astype(f32) + mixed
    combined_whole = all_ranks(combined.astype(bf16).T, core).reshape(WIDTH, frames).astype(f32)
    average = jnp.sum(combined_whole, 0) / WIDTH
    spread = jnp.maximum(jnp.sum(combined_whole * combined_whole, 0) / WIDTH - average * average, 0.0)
    scale = lax.rsqrt(spread + norm_eps)
    middle_whole = ((combined_whole - average) * scale * mix_gain[:, None]).astype(bf16)
    middle_whole = turned(core, middle_whole.reshape(SIDE, SIDE, -1, frames)).reshape(WIDTH, frames)
    middle = ((combined - average[:, None]) * scale[:, None] * mine_of(mix_gain, width_part)).astype(bf16)

    up_proj = lax.dot_general(
        wide[:, :units_part], middle_whole, (((0,), (0,)), ((), ())), preferred_element_type=f32
    )
    hidden = jnp.square(jax.nn.relu(up_proj)).astype(bf16)
    terms = jnp.dot(wide[:, units_part:], hidden, preferred_element_type=f32)
    terms = turned(core, terms.astype(bf16).reshape(SIDE, SIDE, -1, frames))
    terms = terms.reshape(4, 2, width_part, frames)
    kept = lax.dynamic_index_in_dim(terms, core, 1, keepdims=False)
    given = lax.dynamic_index_in_dim(terms, 1 - core, 1, keepdims=False)
    pair = (kept.astype(f32) + partner_of(given).astype(f32)).astype(bf16)
    arrived = lax.all_to_all(pair, "x", 0, 0, tiled=True)
    down_sum = jnp.sum(arrived.astype(f32), 0).T

    final = residual_scale * middle.astype(f32) + down_sum
    sums = jnp.stack([jnp.sum(final, 1), jnp.sum(final * final, 1)])
    copies = jnp.broadcast_to(sums, (SIDE, *sums.shape))
    totals = jnp.sum(lax.all_to_all(copies, TP, 0, 0, tiled=True), 0)
    average = totals[0] / WIDTH
    spread = jnp.maximum(totals[1] / WIDTH - average * average, 0.0)
    scale = lax.rsqrt(spread + norm_eps)
    result = (final - average[:, None]) * scale[:, None] * mine_of(out_gain, width_part)
    return result.astype(bf16)


def solution(mesh):
    split = Mesh(mesh.devices.reshape(8, 8, 4, 2), ALL)
    in_specs = (
        P(FS, TP),
        P(FS, TP),
        P(FS, TP),
        P(),
        P(),
        P(FS, TP),
        P(),
        P(FS, TP),
        P(TP, FS),
        P(),
    )
    return jax.shard_map(layer, mesh=split, in_specs=in_specs, out_specs=P(FS, TP), check_vma=False)
```

```python
import jax
import jax.numpy as jnp
import numpy as np
from jax import lax
from jax.sharding import Mesh
from jax.sharding import PartitionSpec as P


WIDTH = 2048
CHANNELS = 1024
KERNEL = 31
LENGTH = 128
FS = ("z", "y")
TP = ("x", "core")
ALL = ("z", "y", "x", "core")
SIDE = 8


norm_eps = 1e-05
residual_scale = 2.0**0.5
f32 = jnp.float32
bf16 = jnp.bfloat16


def rings(axis_of_core):
    ids = np.arange(SIDE * SIDE * 4 * 2).reshape(SIDE, SIDE, 4, 2)
    out = []
    for x in range(4):
        for core in range(2):
            plane = ids[:, :, x, core]
            out += (plane if axis_of_core[core] == "y" else plane.T).tolist()
    return out


FIRST, SECOND = rings("yz"), rings("zy")


def sent_to_group(shard, groups):
    copies = jnp.broadcast_to(shard, (SIDE, *shard.shape))
    return lax.all_to_all(copies, ALL, 0, 0, axis_index_groups=groups, tiled=True)


def second_axis_pairs(by):
    return [
        (group[i], group[(i + by) % SIDE]) for group in SECOND for i in range(SIDE)
    ]


def doubled(piece):
    for by in (1, 2, 4):
        piece = jnp.concatenate([piece, lax.ppermute(piece, ALL, second_axis_pairs(-by))], 0)
    return piece


def along_x(a, by):
    return lax.ppermute(a, "x", [(i, (i + by) % 4) for i in range(4)])


def partner_of(a):
    return lax.ppermute(a, "core", [(0, 1), (1, 0)])


def turned(core, a):
    return jnp.where(core == 0, a, jnp.swapaxes(a, 0, 1))


def all_ranks(shard, core):
    copies = jnp.broadcast_to(shard, (4, *shard.shape))
    mine = lax.all_to_all(copies, "x", 0, 0, tiled=True)
    other = partner_of(mine)
    both = jnp.stack([jnp.where(core == 0, mine, other), jnp.where(core == 0, other, mine)], 1)
    return both.reshape(SIDE, *shard.shape)


def joined_columns(parts):
    return jnp.moveaxis(parts, 0, 1).reshape(parts.shape[1], -1)


def causal_filter(gated, kernel):
    sequences = gated.shape[0] // LENGTH
    frames = gated.astype(f32).reshape(sequences, LENGTH, gated.shape[1])
    padded = jnp.pad(frames, ((0, 0), (KERNEL - 1, 0), (0, 0)))
    accumulated = jnp.zeros(frames.shape, f32)
    for offset in range(KERNEL):
        accumulated = (
            accumulated + kernel[offset].astype(f32) * padded[:, offset : offset + LENGTH]
        )
    return accumulated.reshape(gated.shape[0], gated.shape[1])


def row_norm_terms(values, entries):
    average = jnp.sum(values, 1, keepdims=True) / entries
    spread = jnp.maximum(jnp.sum(values * values, 1, keepdims=True) / entries - average * average, 0.0)
    return average, lax.rsqrt(spread + norm_eps)


def layer(
    tokens, w_value, w_gate, conv_kernel, conv_gain, w_mix_out, mix_gain, w_up, w_down, out_gain
):
    tp_rank = lax.axis_index(TP)
    core = lax.axis_index("core")
    frames = tokens.shape[0]
    width_part = tokens.shape[1]
    channel_part = w_value.shape[1]
    units_part = w_up.shape[1]

    def mine_of(vector, size):
        return lax.dynamic_slice_in_dim(vector, tp_rank * size, size, vector.ndim - 1)

    own_xt = tokens.T
    mix_rows = w_mix_out.shape[0]
    halves = [w_mix_out[:, :channel_part], w_mix_out[:, channel_part:]]
    shard = jnp.concatenate([w_up, w_down.T, w_value, w_gate, jnp.concatenate(halves, 0)], 1)
    shard = sent_to_group(shard, FIRST).reshape(-1, shard.shape[1])
    at = 2 * units_part
    wide = lax.all_gather(shard[:, :at], ALL, axis=0, tiled=True, axis_index_groups=SECOND)
    value_gate = sent_to_group(shard[:, at : at + 2 * channel_part], SECOND)
    value_gate = value_gate.reshape(WIDTH, 2 * channel_part)
    mix = doubled(shard[None, :, at + 2 * channel_part :])
    mix = jnp.roll(mix, jnp.where(core == 0, lax.axis_index("z"), lax.axis_index("y")), 0)
    mix = mix.reshape(SIDE, SIDE, 2, mix_rows, channel_part)
    mix = turned(core, mix.transpose(0, 1, 3, 2, 4)).reshape(CHANNELS, width_part)

    x_rank = lax.axis_index("x")
    mine = [own_xt, along_x(own_xt, -1), along_x(own_xt, 2), along_x(own_xt, 1)]
    mine = jnp.stack(mine)
    other = partner_of(mine)
    mine, other = jnp.roll(mine, x_rank, 0), jnp.roll(other, x_rank, 0)
    ranks = jnp.stack([jnp.where(core == 0, mine, other), jnp.where(core == 0, other, mine)], 1)
    ranks = turned(core, ranks.reshape(SIDE, SIDE, -1, frames)).reshape(WIDTH, frames)

    both = lax.dot_general(ranks, value_gate, (((0,), (0,)), ((), ())), preferred_element_type=f32)
    values_proj, gate_proj = both[:, :channel_part], both[:, channel_part:]
    gated = (values_proj * jax.nn.sigmoid(gate_proj)).astype(bf16)
    filtered = causal_filter(gated, mine_of(conv_kernel, channel_part))
    filtered_whole = joined_columns(all_ranks(filtered.astype(bf16), core)).astype(f32)
    average, scale = row_norm_terms(filtered_whole, CHANNELS)
    activated = jax.nn.silu((filtered_whole - average) * scale * conv_gain).astype(bf16)

    mixed = jnp.dot(activated, mix, preferred_element_type=f32)
    combined = residual_scale * tokens.astype(f32) + mixed
    combined_whole = all_ranks(combined.astype(bf16).T, core).reshape(WIDTH, frames).astype(f32)
    average = jnp.sum(combined_whole, 0) / WIDTH
    spread = jnp.maximum(jnp.sum(combined_whole * combined_whole, 0) / WIDTH - average * average, 0.0)
    scale = lax.rsqrt(spread + norm_eps)
    middle_whole = ((combined_whole - average) * scale * mix_gain[:, None]).astype(bf16)
    middle_whole = turned(core, middle_whole.reshape(SIDE, SIDE, -1, frames)).reshape(WIDTH, frames)
    middle = ((combined - average[:, None]) * scale[:, None] * mine_of(mix_gain, width_part)).astype(bf16)

    up_proj = lax.dot_general(
        wide[:, :units_part], middle_whole, (((0,), (0,)), ((), ())), preferred_element_type=f32
    )
    hidden = jnp.square(jax.nn.relu(up_proj)).astype(bf16)
    terms = jnp.dot(wide[:, units_part:], hidden, preferred_element_type=f32)
    terms = turned(core, terms.astype(bf16).reshape(SIDE, SIDE, -1, frames))
    terms = terms.reshape(4, 2, width_part, frames)
    kept = lax.dynamic_index_in_dim(terms, core, 1, keepdims=False)
    given = lax.dynamic_index_in_dim(terms, 1 - core, 1, keepdims=False)
    pair = (kept.astype(f32) + partner_of(given).astype(f32)).astype(bf16)
    arrived = lax.all_to_all(pair, "x", 0, 0, tiled=True)
    down_sum = jnp.sum(arrived.astype(f32), 0).T

    final = residual_scale * middle.astype(f32) + down_sum
    sums = jnp.stack([jnp.sum(final, 1), jnp.sum(final * final, 1)])
    copies = jnp.broadcast_to(sums, (SIDE, *sums.shape))
    totals = jnp.sum(lax.all_to_all(copies, TP, 0, 0, tiled=True), 0)
    average = totals[0] / WIDTH
    spread = jnp.maximum(totals[1] / WIDTH - average * average, 0.0)
    scale = lax.rsqrt(spread + norm_eps)
    result = (final - average[:, None]) * scale[:, None] * mine_of(out_gain, width_part)
    return result.astype(bf16)


def solution(mesh):
    split = Mesh(mesh.devices.reshape(8, 8, 4, 2), ALL)
    in_specs = (
        P(FS, TP),
        P(FS, TP),
        P(FS, TP),
        P(),
        P(),
        P(FS, TP),
        P(),
        P(FS, TP),
        P(TP, FS),
        P(),
    )
    return jax.shard_map(layer, mesh=split, in_specs=in_specs, out_specs=P(FS, TP), check_vma=False)
```

```python
import jax
import jax.numpy as jnp
import numpy as np
from jax import lax
from jax.sharding import Mesh
from jax.sharding import PartitionSpec as P


WIDTH = 2048
CHANNELS = 1024
KERNEL = 31
LENGTH = 128
FS = ("z", "y")
TP = ("x", "core")
ALL = ("z", "y", "x", "core")
SIDE = 8


norm_eps = 1e-05
residual_scale = 2.0**0.5
f32 = jnp.float32
bf16 = jnp.bfloat16


def rings(axis_of_core):
    ids = np.arange(SIDE * SIDE * 4 * 2).reshape(SIDE, SIDE, 4, 2)
    out = []
    for x in range(4):
        for core in range(2):
            plane = ids[:, :, x, core]
            out += (plane if axis_of_core[core] == "y" else plane.T).tolist()
    return out


FIRST, SECOND = rings("yz"), rings("zy")
FOURS = [group[parity::2] for group in FIRST for parity in range(2)]
PAIRS = [(a, group[i ^ 1]) for group in FIRST for i, a in enumerate(group)]


def sent_to_group(shard, groups):
    copies = jnp.broadcast_to(shard, (SIDE, *shard.shape))
    return lax.all_to_all(copies, ALL, 0, 0, axis_index_groups=groups, tiled=True)


def along_x(a, by):
    return lax.ppermute(a, "x", [(i, (i + by) % 4) for i in range(4)])


def partner_of(a):
    return lax.ppermute(a, "core", [(0, 1), (1, 0)])


def turned(core, a):
    return jnp.where(core == 0, a, jnp.swapaxes(a, 0, 1))


def all_ranks(shard, core):
    copies = jnp.broadcast_to(shard, (4, *shard.shape))
    mine = lax.all_to_all(copies, "x", 0, 0, tiled=True)
    other = partner_of(mine)
    both = jnp.stack([jnp.where(core == 0, mine, other), jnp.where(core == 0, other, mine)], 1)
    return both.reshape(SIDE, *shard.shape)


def joined_columns(parts):
    return jnp.moveaxis(parts, 0, 1).reshape(parts.shape[1], -1)


def causal_filter(gated, kernel):
    sequences = gated.shape[0] // LENGTH
    frames = gated.astype(f32).reshape(sequences, LENGTH, gated.shape[1])
    padded = jnp.pad(frames, ((0, 0), (KERNEL - 1, 0), (0, 0)))
    accumulated = jnp.zeros(frames.shape, f32)
    for offset in range(KERNEL):
        accumulated = (
            accumulated + kernel[offset].astype(f32) * padded[:, offset : offset + LENGTH]
        )
    return accumulated.reshape(gated.shape[0], gated.shape[1])


def row_norm_terms(values, entries):
    average = jnp.sum(values, 1, keepdims=True) / entries
    spread = jnp.maximum(jnp.sum(values * values, 1, keepdims=True) / entries - average * average, 0.0)
    return average, lax.rsqrt(spread + norm_eps)


def layer(
    tokens, w_value, w_gate, conv_kernel, conv_gain, w_mix_out, mix_gain, w_up, w_down, out_gain
):
    tp_rank = lax.axis_index(TP)
    core = lax.axis_index("core")
    frames = tokens.shape[0]
    width_part = tokens.shape[1]
    channel_part = w_value.shape[1]
    units_part = w_up.shape[1]

    def mine_of(vector, size):
        return lax.dynamic_slice_in_dim(vector, tp_rank * size, size, vector.ndim - 1)

    wide = jnp.concatenate([w_up, w_down.T], 1)
    place = jnp.where(core == 0, lax.axis_index("y"), lax.axis_index("z"))
    met = lax.ppermute(wide, ALL, PAIRS)
    even = place % 2 == 0
    wide = jnp.concatenate([jnp.where(even, wide, met), jnp.where(even, met, wide)], 0)
    wide = lax.all_gather(wide, ALL, axis=0, tiled=True, axis_index_groups=FOURS)
    wide = lax.all_gather(wide, ALL, axis=0, tiled=True, axis_index_groups=SECOND)

    mix_rows = w_mix_out.shape[0]
    halves = [w_mix_out[:, :channel_part], w_mix_out[:, channel_part:]]
    small = jnp.concatenate([w_value, w_gate, jnp.concatenate(halves, 0)], 1)
    small = sent_to_group(small, FIRST).reshape(-1, small.shape[1])
    small = sent_to_group(small, SECOND)
    value_gate = small[:, :, : 2 * channel_part].reshape(WIDTH, 2 * channel_part)
    mix = small[:, :, 2 * channel_part :].reshape(SIDE, SIDE, 2, mix_rows, channel_part)
    mix = turned(core, mix.transpose(0, 1, 3, 2, 4)).reshape(CHANNELS, width_part)

    x_rank = lax.axis_index("x")
    own_xt = tokens.T
    parts = [own_xt, along_x(own_xt, -1), along_x(own_xt, 2), along_x(own_xt, 1)]
    mine = jnp.stack(parts)
    other = partner_of(mine)
    mine, other = jnp.roll(mine, x_rank, 0), jnp.roll(other, x_rank, 0)
    ranks = jnp.stack([jnp.where(core == 0, mine, other), jnp.where(core == 0, other, mine)], 1)
    ranks = turned(core, ranks.reshape(SIDE, SIDE, -1, frames)).reshape(WIDTH, frames)

    both = lax.dot_general(ranks, value_gate, (((0,), (0,)), ((), ())), preferred_element_type=f32)
    values_proj, gate_proj = both[:, :channel_part], both[:, channel_part:]
    gated = (values_proj * jax.nn.sigmoid(gate_proj)).astype(bf16)
    filtered = causal_filter(gated, mine_of(conv_kernel, channel_part))
    filtered_whole = joined_columns(all_ranks(filtered.astype(bf16), core)).astype(f32)
    average, scale = row_norm_terms(filtered_whole, CHANNELS)
    activated = jax.nn.silu((filtered_whole - average) * scale * conv_gain).astype(bf16)

    mixed = jnp.dot(activated, mix, preferred_element_type=f32)
    combined = residual_scale * tokens.astype(f32) + mixed
    combined_whole = all_ranks(combined.astype(bf16).T, core).reshape(WIDTH, frames).astype(f32)
    average = jnp.sum(combined_whole, 0) / WIDTH
    spread = jnp.maximum(jnp.sum(combined_whole * combined_whole, 0) / WIDTH - average * average, 0.0)
    scale = lax.rsqrt(spread + norm_eps)
    middle_whole = ((combined_whole - average) * scale * mix_gain[:, None]).astype(bf16)
    middle_whole = turned(core, middle_whole.reshape(SIDE, SIDE, -1, frames)).reshape(WIDTH, frames)
    middle = ((combined - average[:, None]) * scale[:, None] * mine_of(mix_gain, width_part)).astype(bf16)

    up_proj = lax.dot_general(
        wide[:, :units_part], middle_whole, (((0,), (0,)), ((), ())), preferred_element_type=f32
    )
    hidden = jnp.square(jax.nn.relu(up_proj)).astype(bf16)
    terms = jnp.dot(wide[:, units_part:], hidden, preferred_element_type=f32)
    terms = turned(core, terms.astype(bf16).reshape(SIDE, SIDE, -1, frames))
    terms = terms.reshape(4, 2, width_part, frames)
    kept = lax.dynamic_index_in_dim(terms, core, 1, keepdims=False)
    given = lax.dynamic_index_in_dim(terms, 1 - core, 1, keepdims=False)
    pair = (kept.astype(f32) + partner_of(given).astype(f32)).astype(bf16)
    arrived = lax.all_to_all(pair, "x", 0, 0, tiled=True)
    down_sum = jnp.sum(arrived.astype(f32), 0).T

    final = residual_scale * middle.astype(f32) + down_sum
    sums = jnp.stack([jnp.sum(final, 1), jnp.sum(final * final, 1)])
    copies = jnp.broadcast_to(sums, (SIDE, *sums.shape))
    totals = jnp.sum(lax.all_to_all(copies, TP, 0, 0, tiled=True), 0)
    average = totals[0] / WIDTH
    spread = jnp.maximum(totals[1] / WIDTH - average * average, 0.0)
    scale = lax.rsqrt(spread + norm_eps)
    result = (final - average[:, None]) * scale[:, None] * mine_of(out_gain, width_part)
    return result.astype(bf16)


def solution(mesh):
    split = Mesh(mesh.devices.reshape(8, 8, 4, 2), ALL)
    in_specs = (
        P(FS, TP),
        P(FS, TP),
        P(FS, TP),
        P(),
        P(),
        P(FS, TP),
        P(),
        P(FS, TP),
        P(TP, FS),
        P(),
    )
    return jax.shard_map(layer, mesh=split, in_specs=in_specs, out_specs=P(FS, TP), check_vma=False)
```

```python
import jax
import jax.numpy as jnp
import numpy as np
from jax import lax
from jax.experimental import pallas as pl
from jax.experimental.pallas import tpu as pltpu
from jax.sharding import Mesh
from jax.sharding import PartitionSpec as P


WIDTH = 2048
CHANNELS = 1024
KERNEL = 31
LENGTH = 128
FS = ("z", "y")
TP = ("x", "core")
ALL = ("z", "y", "x", "core")
SIDE = 8


norm_eps = 1e-05
residual_scale = 2.0**0.5
f32 = jnp.float32
bf16 = jnp.bfloat16


def rings(axis_of_core):
    ids = np.arange(SIDE * SIDE * 4 * 2).reshape(SIDE, SIDE, 4, 2)
    out = []
    for x in range(4):
        for core in range(2):
            plane = ids[:, :, x, core]
            out += (plane if axis_of_core[core] == "y" else plane.T).tolist()
    return out


FIRST, SECOND = rings("yz"), rings("zy")


def pairs(groups, by):
    return [(group[i], group[(i + by) % SIDE]) for group in groups for i in range(SIDE)]


def place_blocks(place_ref, *refs):
    blocks, out, sems = refs[:SIDE], refs[SIDE], refs[SIDE + 1]
    rows = blocks[0].shape[0]
    copies = []
    for i, block in enumerate(blocks):
        start = pl.multiple_of(lax.rem(place_ref[0] + i, SIDE) * rows, rows)
        copies.append(pltpu.make_async_copy(block, out.at[pl.ds(start, rows)], sems.at[i]))
        copies[-1].start()
    for copy in copies:
        copy.wait()


def in_place(blocks, place):
    rows, columns = blocks[0].shape
    size = SIDE * rows * columns
    return pl.pallas_call(
        place_blocks,
        out_shape=jax.ShapeDtypeStruct((SIDE * rows, columns), blocks[0].dtype),
        in_specs=[pl.BlockSpec(memory_space=pltpu.SMEM)] + [pl.BlockSpec(memory_space=pl.ANY)] * SIDE,
        out_specs=pl.BlockSpec(memory_space=pl.ANY),
        scratch_shapes=[pltpu.SemaphoreType.DMA((SIDE,))],
        cost_estimate=pl.CostEstimate(flops=size, bytes_accessed=4 * size, transcendentals=0),
        compiler_params=pltpu.CompilerParams(vmem_limit_bytes=1 << 20),
        name="place_blocks",
    )(place.astype(jnp.int32).reshape(1), *blocks)


def sent_to_group(shard, groups):
    copies = jnp.broadcast_to(shard, (SIDE, *shard.shape))
    return lax.all_to_all(copies, ALL, 0, 0, axis_index_groups=groups, tiled=True)


def along_x(a, by):
    return lax.ppermute(a, "x", [(i, (i + by) % 4) for i in range(4)])


def partner_of(a):
    return lax.ppermute(a, "core", [(0, 1), (1, 0)])


def turned(core, a):
    return jnp.where(core == 0, a, jnp.swapaxes(a, 0, 1))


def all_ranks(shard, core):
    copies = jnp.broadcast_to(shard, (4, *shard.shape))
    mine = lax.all_to_all(copies, "x", 0, 0, tiled=True)
    other = partner_of(mine)
    both = jnp.stack([jnp.where(core == 0, mine, other), jnp.where(core == 0, other, mine)], 1)
    return both.reshape(SIDE, *shard.shape)


def joined_columns(parts):
    return jnp.moveaxis(parts, 0, 1).reshape(parts.shape[1], -1)


def causal_filter(gated, kernel):
    sequences = gated.shape[0] // LENGTH
    frames = gated.astype(f32).reshape(sequences, LENGTH, gated.shape[1])
    padded = jnp.pad(frames, ((0, 0), (KERNEL - 1, 0), (0, 0)))
    accumulated = jnp.zeros(frames.shape, f32)
    for offset in range(KERNEL):
        accumulated = (
            accumulated + kernel[offset].astype(f32) * padded[:, offset : offset + LENGTH]
        )
    return accumulated.reshape(gated.shape[0], gated.shape[1])


def row_norm_terms(values, entries):
    average = jnp.sum(values, 1, keepdims=True) / entries
    spread = jnp.maximum(jnp.sum(values * values, 1, keepdims=True) / entries - average * average, 0.0)
    return average, lax.rsqrt(spread + norm_eps)


def layer(
    tokens, w_value, w_gate, conv_kernel, conv_gain, w_mix_out, mix_gain, w_up, w_down, out_gain
):
    tp_rank = lax.axis_index(TP)
    core = lax.axis_index("core")
    frames = tokens.shape[0]
    width_part = tokens.shape[1]
    channel_part = w_value.shape[1]
    units_part = w_up.shape[1]

    def mine_of(vector, size):
        return lax.dynamic_slice_in_dim(vector, tp_rank * size, size, vector.ndim - 1)

    wide = jnp.concatenate([w_up, w_down.T], 1)
    place = jnp.where(core == 0, lax.axis_index("y"), lax.axis_index("z"))
    blocks = [wide] + [lax.ppermute(wide, ALL, pairs(FIRST, -by)) for by in range(1, SIDE)]
    wide = in_place(blocks, place)
    wide = lax.all_gather(wide, ALL, axis=0, tiled=True, axis_index_groups=SECOND)

    mix_rows = w_mix_out.shape[0]
    halves = [w_mix_out[:, :channel_part], w_mix_out[:, channel_part:]]
    small = jnp.concatenate([w_value, w_gate, jnp.concatenate(halves, 0)], 1)
    small = sent_to_group(small, FIRST).reshape(-1, small.shape[1])
    small = sent_to_group(small, SECOND)
    value_gate = small[:, :, : 2 * channel_part].reshape(WIDTH, 2 * channel_part)
    mix = small[:, :, 2 * channel_part :].reshape(SIDE, SIDE, 2, mix_rows, channel_part)
    mix = turned(core, mix.transpose(0, 1, 3, 2, 4)).reshape(CHANNELS, width_part)

    x_rank = lax.axis_index("x")
    own_xt = tokens.T
    parts = [own_xt, along_x(own_xt, -1), along_x(own_xt, 2), along_x(own_xt, 1)]
    mine = jnp.stack(parts)
    other = partner_of(mine)
    mine, other = jnp.roll(mine, x_rank, 0), jnp.roll(other, x_rank, 0)
    ranks = jnp.stack([jnp.where(core == 0, mine, other), jnp.where(core == 0, other, mine)], 1)
    ranks = turned(core, ranks.reshape(SIDE, SIDE, -1, frames)).reshape(WIDTH, frames)

    both = lax.dot_general(ranks, value_gate, (((0,), (0,)), ((), ())), preferred_element_type=f32)
    values_proj, gate_proj = both[:, :channel_part], both[:, channel_part:]
    gated = (values_proj * jax.nn.sigmoid(gate_proj)).astype(bf16)
    filtered = causal_filter(gated, mine_of(conv_kernel, channel_part))
    filtered_whole = joined_columns(all_ranks(filtered.astype(bf16), core)).astype(f32)
    average, scale = row_norm_terms(filtered_whole, CHANNELS)
    activated = jax.nn.silu((filtered_whole - average) * scale * conv_gain).astype(bf16)

    mixed = jnp.dot(activated, mix, preferred_element_type=f32)
    combined = residual_scale * tokens.astype(f32) + mixed
    combined_whole = all_ranks(combined.astype(bf16).T, core).reshape(WIDTH, frames).astype(f32)
    average = jnp.sum(combined_whole, 0) / WIDTH
    spread = jnp.maximum(jnp.sum(combined_whole * combined_whole, 0) / WIDTH - average * average, 0.0)
    scale = lax.rsqrt(spread + norm_eps)
    middle_whole = ((combined_whole - average) * scale * mix_gain[:, None]).astype(bf16)
    middle_whole = turned(core, middle_whole.reshape(SIDE, SIDE, -1, frames)).reshape(WIDTH, frames)
    middle = ((combined - average[:, None]) * scale[:, None] * mine_of(mix_gain, width_part)).astype(bf16)

    up_proj = lax.dot_general(
        wide[:, :units_part], middle_whole, (((0,), (0,)), ((), ())), preferred_element_type=f32
    )
    hidden = jnp.square(jax.nn.relu(up_proj)).astype(bf16)
    terms = jnp.dot(wide[:, units_part:], hidden, preferred_element_type=f32)
    terms = turned(core, terms.astype(bf16).reshape(SIDE, SIDE, -1, frames))
    terms = terms.reshape(4, 2, width_part, frames)
    kept = lax.dynamic_index_in_dim(terms, core, 1, keepdims=False)
    given = lax.dynamic_index_in_dim(terms, 1 - core, 1, keepdims=False)
    pair = (kept.astype(f32) + partner_of(given).astype(f32)).astype(bf16)
    arrived = lax.all_to_all(pair, "x", 0, 0, tiled=True)
    down_sum = jnp.sum(arrived.astype(f32), 0).T

    final = residual_scale * middle.astype(f32) + down_sum
    sums = jnp.stack([jnp.sum(final, 1), jnp.sum(final * final, 1)])
    copies = jnp.broadcast_to(sums, (SIDE, *sums.shape))
    totals = jnp.sum(lax.all_to_all(copies, TP, 0, 0, tiled=True), 0)
    average = totals[0] / WIDTH
    spread = jnp.maximum(totals[1] / WIDTH - average * average, 0.0)
    scale = lax.rsqrt(spread + norm_eps)
    result = (final - average[:, None]) * scale[:, None] * mine_of(out_gain, width_part)
    return result.astype(bf16)


def solution(mesh):
    split = Mesh(mesh.devices.reshape(8, 8, 4, 2), ALL)
    in_specs = (
        P(FS, TP),
        P(FS, TP),
        P(FS, TP),
        P(),
        P(),
        P(FS, TP),
        P(),
        P(FS, TP),
        P(TP, FS),
        P(),
    )
    return jax.shard_map(layer, mesh=split, in_specs=in_specs, out_specs=P(FS, TP), check_vma=False)
```

```python
import jax
import jax.numpy as jnp
import numpy as np
from jax import lax
from jax.sharding import Mesh
from jax.sharding import PartitionSpec as P


WIDTH = 2048
CHANNELS = 1024
KERNEL = 31
LENGTH = 128
FS = ("z", "y")
TP = ("x", "core")
ALL = ("z", "y", "x", "core")
SIDE = 8


norm_eps = 1e-05
residual_scale = 2.0**0.5
f32 = jnp.float32
bf16 = jnp.bfloat16


def rings(axis_of_core):
    ids = np.arange(SIDE * SIDE * 4 * 2).reshape(SIDE, SIDE, 4, 2)
    out = []
    for x in range(4):
        for core in range(2):
            plane = ids[:, :, x, core]
            out += (plane if axis_of_core[core] == "y" else plane.T).tolist()
    return out


FIRST, SECOND = rings("yz"), rings("zy")


def sent_to_group(shard, groups):
    copies = jnp.broadcast_to(shard, (SIDE, *shard.shape))
    return lax.all_to_all(copies, ALL, 0, 0, axis_index_groups=groups, tiled=True)


def along_x(a, by):
    return lax.ppermute(a, "x", [(i, (i + by) % 4) for i in range(4)])


def partner_of(a):
    return lax.ppermute(a, "core", [(0, 1), (1, 0)])


def turned(core, a):
    return jnp.where(core == 0, a, jnp.swapaxes(a, 0, 1))


def all_ranks(shard, core):
    copies = jnp.broadcast_to(shard, (4, *shard.shape))
    mine = lax.all_to_all(copies, "x", 0, 0, tiled=True)
    other = partner_of(mine)
    both = jnp.stack([jnp.where(core == 0, mine, other), jnp.where(core == 0, other, mine)], 1)
    return both.reshape(SIDE, *shard.shape)


def joined_columns(parts):
    return jnp.moveaxis(parts, 0, 1).reshape(parts.shape[1], -1)


def causal_filter(gated, kernel):
    sequences = gated.shape[0] // LENGTH
    frames = gated.astype(f32).reshape(sequences, LENGTH, gated.shape[1])
    padded = jnp.pad(frames, ((0, 0), (KERNEL - 1, 0), (0, 0)))
    accumulated = jnp.zeros(frames.shape, f32)
    for offset in range(KERNEL):
        accumulated = (
            accumulated + kernel[offset].astype(f32) * padded[:, offset : offset + LENGTH]
        )
    return accumulated.reshape(gated.shape[0], gated.shape[1])


def row_norm_terms(values, entries):
    average = jnp.sum(values, 1, keepdims=True) / entries
    spread = jnp.maximum(jnp.sum(values * values, 1, keepdims=True) / entries - average * average, 0.0)
    return average, lax.rsqrt(spread + norm_eps)


def layer(
    tokens, w_value, w_gate, conv_kernel, conv_gain, w_mix_out, mix_gain, w_up, w_down, out_gain
):
    tp_rank = lax.axis_index(TP)
    core = lax.axis_index("core")
    frames = tokens.shape[0]
    width_part = tokens.shape[1]
    channel_part = w_value.shape[1]
    units_part = w_up.shape[1]

    def mine_of(vector, size):
        return lax.dynamic_slice_in_dim(vector, tp_rank * size, size, vector.ndim - 1)

    wide = jnp.concatenate([w_up, w_down.T], 1)
    wide = lax.all_gather(wide, FS, axis=0, tiled=True)

    mix_rows = w_mix_out.shape[0]
    halves = [w_mix_out[:, :channel_part], w_mix_out[:, channel_part:]]
    small = jnp.concatenate([w_value, w_gate, jnp.concatenate(halves, 0)], 1)
    small = sent_to_group(small, FIRST).reshape(-1, small.shape[1])
    small = sent_to_group(small, SECOND)
    value_gate = small[:, :, : 2 * channel_part].reshape(WIDTH, 2 * channel_part)
    mix = small[:, :, 2 * channel_part :].reshape(SIDE, SIDE, 2, mix_rows, channel_part)
    mix = turned(core, mix.transpose(0, 1, 3, 2, 4)).reshape(CHANNELS, width_part)

    x_rank = lax.axis_index("x")
    own_xt = tokens.T
    parts = [own_xt, along_x(own_xt, -1), along_x(own_xt, 2), along_x(own_xt, 1)]
    mine = jnp.stack(parts)
    other = partner_of(mine)
    mine, other = jnp.roll(mine, x_rank, 0), jnp.roll(other, x_rank, 0)
    ranks = jnp.stack([jnp.where(core == 0, mine, other), jnp.where(core == 0, other, mine)], 1)
    ranks = turned(core, ranks.reshape(SIDE, SIDE, -1, frames)).reshape(WIDTH, frames)

    both = lax.dot_general(ranks, value_gate, (((0,), (0,)), ((), ())), preferred_element_type=f32)
    values_proj, gate_proj = both[:, :channel_part], both[:, channel_part:]
    gated = (values_proj * jax.nn.sigmoid(gate_proj)).astype(bf16)
    filtered = causal_filter(gated, mine_of(conv_kernel, channel_part))
    filtered_whole = joined_columns(all_ranks(filtered.astype(bf16), core)).astype(f32)
    average, scale = row_norm_terms(filtered_whole, CHANNELS)
    activated = jax.nn.silu((filtered_whole - average) * scale * conv_gain).astype(bf16)

    mixed = jnp.dot(activated, mix, preferred_element_type=f32)
    combined = residual_scale * tokens.astype(f32) + mixed
    combined_whole = all_ranks(combined.astype(bf16).T, core).reshape(WIDTH, frames).astype(f32)
    average = jnp.sum(combined_whole, 0) / WIDTH
    spread = jnp.maximum(jnp.sum(combined_whole * combined_whole, 0) / WIDTH - average * average, 0.0)
    scale = lax.rsqrt(spread + norm_eps)
    middle_whole = ((combined_whole - average) * scale * mix_gain[:, None]).astype(bf16)
    middle = ((combined - average[:, None]) * scale[:, None] * mine_of(mix_gain, width_part)).astype(bf16)

    up_proj = lax.dot_general(
        wide[:, :units_part], middle_whole, (((0,), (0,)), ((), ())), preferred_element_type=f32
    )
    hidden = jnp.square(jax.nn.relu(up_proj)).astype(bf16)
    terms = jnp.dot(wide[:, units_part:], hidden, preferred_element_type=f32)
    terms = terms.astype(bf16).reshape(4, 2, width_part, frames)
    kept = lax.dynamic_index_in_dim(terms, core, 1, keepdims=False)
    given = lax.dynamic_index_in_dim(terms, 1 - core, 1, keepdims=False)
    pair = (kept.astype(f32) + partner_of(given).astype(f32)).astype(bf16)
    arrived = lax.all_to_all(pair, "x", 0, 0, tiled=True)
    down_sum = jnp.sum(arrived.astype(f32), 0).T

    final = residual_scale * middle.astype(f32) + down_sum
    sums = jnp.stack([jnp.sum(final, 1), jnp.sum(final * final, 1)])
    copies = jnp.broadcast_to(sums, (SIDE, *sums.shape))
    totals = jnp.sum(lax.all_to_all(copies, TP, 0, 0, tiled=True), 0)
    average = totals[0] / WIDTH
    spread = jnp.maximum(totals[1] / WIDTH - average * average, 0.0)
    scale = lax.rsqrt(spread + norm_eps)
    result = (final - average[:, None]) * scale[:, None] * mine_of(out_gain, width_part)
    return result.astype(bf16)


def solution(mesh):
    split = Mesh(mesh.devices.reshape(8, 8, 4, 2), ALL)
    in_specs = (
        P(FS, TP),
        P(FS, TP),
        P(FS, TP),
        P(),
        P(),
        P(FS, TP),
        P(),
        P(FS, TP),
        P(TP, FS),
        P(),
    )
    return jax.shard_map(layer, mesh=split, in_specs=in_specs, out_specs=P(FS, TP), check_vma=False)
```

```python
import jax
import jax.numpy as jnp
import numpy as np
from jax import lax
from jax.sharding import Mesh
from jax.sharding import PartitionSpec as P


WIDTH = 2048
CHANNELS = 1024
KERNEL = 31
LENGTH = 128
FS = ("z", "y")
TP = ("x", "core")
ALL = ("z", "y", "x", "core")
SIDE = 8


norm_eps = 1e-05
residual_scale = 2.0**0.5
f32 = jnp.float32
bf16 = jnp.bfloat16


def rings(axis_of_core):
    ids = np.arange(SIDE * SIDE * 4 * 2).reshape(SIDE, SIDE, 4, 2)
    out = []
    for x in range(4):
        for core in range(2):
            plane = ids[:, :, x, core]
            out += (plane if axis_of_core[core] == "y" else plane.T).tolist()
    return out


FIRST, SECOND = rings("yz"), rings("zy")


def sent_to_group(shard, groups):
    copies = jnp.broadcast_to(shard, (SIDE, *shard.shape))
    return lax.all_to_all(copies, ALL, 0, 0, axis_index_groups=groups, tiled=True)


def along_x(a, by):
    return lax.ppermute(a, "x", [(i, (i + by) % 4) for i in range(4)])


def partner_of(a):
    return lax.ppermute(a, "core", [(0, 1), (1, 0)])


def turned(core, a):
    return jnp.where(core == 0, a, jnp.swapaxes(a, 0, 1))


def all_ranks(shard, core):
    copies = jnp.broadcast_to(shard, (4, *shard.shape))
    mine = lax.all_to_all(copies, "x", 0, 0, tiled=True)
    other = partner_of(mine)
    both = jnp.stack([jnp.where(core == 0, mine, other), jnp.where(core == 0, other, mine)], 1)
    return both.reshape(SIDE, *shard.shape)


def joined_columns(parts):
    return jnp.moveaxis(parts, 0, 1).reshape(parts.shape[1], -1)


def causal_filter(gated, kernel):
    sequences = gated.shape[0] // LENGTH
    frames = gated.astype(f32).reshape(sequences, LENGTH, gated.shape[1])
    padded = jnp.pad(frames, ((0, 0), (KERNEL - 1, 0), (0, 0)))
    accumulated = jnp.zeros(frames.shape, f32)
    for offset in range(KERNEL):
        accumulated = (
            accumulated + kernel[offset].astype(f32) * padded[:, offset : offset + LENGTH]
        )
    return accumulated.reshape(gated.shape[0], gated.shape[1])


def row_norm_terms(values, entries):
    average = jnp.sum(values, 1, keepdims=True) / entries
    spread = jnp.maximum(jnp.sum(values * values, 1, keepdims=True) / entries - average * average, 0.0)
    return average, lax.rsqrt(spread + norm_eps)


def layer(
    tokens, w_value, w_gate, conv_kernel, conv_gain, w_mix_out, mix_gain, w_up, w_down, out_gain
):
    tp_rank = lax.axis_index(TP)
    core = lax.axis_index("core")
    frames = tokens.shape[0]
    width_part = tokens.shape[1]
    channel_part = w_value.shape[1]
    units_part = w_up.shape[1]

    def mine_of(vector, size):
        return lax.dynamic_slice_in_dim(vector, tp_rank * size, size, vector.ndim - 1)

    own_mix_gain = mine_of(mix_gain, width_part)
    own_out_gain = mine_of(out_gain, width_part)
    own_xt = tokens.T
    mix_rows = w_mix_out.shape[0]
    halves = [w_mix_out[:, :channel_part], w_mix_out[:, channel_part:]]
    shard = jnp.concatenate([w_up, w_down.T, w_value, w_gate, jnp.concatenate(halves, 0)], 1)
    shard = sent_to_group(shard, FIRST).reshape(-1, shard.shape[1])
    at = 2 * units_part
    wide = lax.all_gather(shard[:, :at], ALL, axis=0, tiled=True, axis_index_groups=SECOND)
    small = sent_to_group(shard[:, at:], SECOND)
    value_gate = small[:, :, : 2 * channel_part].reshape(WIDTH, 2 * channel_part)
    mix = small[:, :, 2 * channel_part :].reshape(SIDE, SIDE, 2, mix_rows, channel_part)
    mix = turned(core, mix.transpose(0, 1, 3, 2, 4)).reshape(CHANNELS, width_part)

    x_rank = lax.axis_index("x")
    mine = [own_xt, along_x(own_xt, -1), along_x(own_xt, 2), along_x(own_xt, 1)]
    mine = jnp.stack(mine)
    other = partner_of(mine)
    mine, other = jnp.roll(mine, x_rank, 0), jnp.roll(other, x_rank, 0)
    ranks = jnp.stack([jnp.where(core == 0, mine, other), jnp.where(core == 0, other, mine)], 1)
    ranks = turned(core, ranks.reshape(SIDE, SIDE, -1, frames)).reshape(WIDTH, frames)

    both = lax.dot_general(ranks, value_gate, (((0,), (0,)), ((), ())), preferred_element_type=f32)
    values_proj, gate_proj = both[:, :channel_part], both[:, channel_part:]
    gated = (values_proj * jax.nn.sigmoid(gate_proj)).astype(bf16)
    filtered = causal_filter(gated, mine_of(conv_kernel, channel_part))
    filtered_whole = joined_columns(all_ranks(filtered.astype(bf16), core)).astype(f32)
    average, scale = row_norm_terms(filtered_whole, CHANNELS)
    activated = jax.nn.silu((filtered_whole - average) * scale * conv_gain).astype(bf16)

    mixed = jnp.dot(activated, mix, preferred_element_type=f32)
    combined = residual_scale * tokens.astype(f32) + mixed
    combined_whole = all_ranks(combined.astype(bf16).T, core).reshape(WIDTH, frames).astype(f32)
    average = jnp.sum(combined_whole, 0) / WIDTH
    spread = jnp.maximum(jnp.sum(combined_whole * combined_whole, 0) / WIDTH - average * average, 0.0)
    scale = lax.rsqrt(spread + norm_eps)
    middle_whole = ((combined_whole - average) * scale * mix_gain[:, None]).astype(bf16)
    middle_whole = turned(core, middle_whole.reshape(SIDE, SIDE, -1, frames)).reshape(WIDTH, frames)
    middle = ((combined - average[:, None]) * scale[:, None] * own_mix_gain).astype(bf16)

    up_proj = lax.dot_general(
        wide[:, :units_part], middle_whole, (((0,), (0,)), ((), ())), preferred_element_type=f32
    )
    hidden = jnp.square(jax.nn.relu(up_proj)).astype(bf16)
    terms = jnp.dot(wide[:, units_part:], hidden, preferred_element_type=f32)
    terms = turned(core, terms.astype(bf16).reshape(SIDE, SIDE, -1, frames))
    terms = terms.reshape(4, 2, width_part, frames)
    kept = lax.dynamic_index_in_dim(terms, core, 1, keepdims=False)
    given = lax.dynamic_index_in_dim(terms, 1 - core, 1, keepdims=False)
    pair = (kept.astype(f32) + partner_of(given).astype(f32)).astype(bf16)
    arrived = lax.all_to_all(pair, "x", 0, 0, tiled=True)
    down_sum = jnp.sum(arrived.astype(f32), 0).T

    final = residual_scale * middle.astype(f32) + down_sum
    sums = jnp.stack([jnp.sum(final, 1), jnp.sum(final * final, 1)])
    copies = jnp.broadcast_to(sums, (SIDE, *sums.shape))
    totals = jnp.sum(lax.all_to_all(copies, TP, 0, 0, tiled=True), 0)
    average = totals[0] / WIDTH
    spread = jnp.maximum(totals[1] / WIDTH - average * average, 0.0)
    scale = lax.rsqrt(spread + norm_eps)
    result = (final - average[:, None]) * scale[:, None] * own_out_gain
    return result.astype(bf16)


def solution(mesh):
    split = Mesh(mesh.devices.reshape(8, 8, 4, 2), ALL)
    in_specs = (
        P(FS, TP),
        P(FS, TP),
        P(FS, TP),
        P(),
        P(),
        P(FS, TP),
        P(),
        P(FS, TP),
        P(TP, FS),
        P(),
    )
    return jax.shard_map(layer, mesh=split, in_specs=in_specs, out_specs=P(FS, TP), check_vma=False)
```

```python
import jax
import jax.numpy as jnp
import numpy as np
from jax import lax
from jax.experimental import pallas as pl
from jax.experimental.pallas import tpu as pltpu
from jax.sharding import Mesh
from jax.sharding import PartitionSpec as P


WIDTH = 2048
CHANNELS = 1024
KERNEL = 31
LENGTH = 128
FS = ("z", "y")
TP = ("x", "core")
ALL = ("z", "y", "x", "core")
SIDE = 8


norm_eps = 1e-05
residual_scale = 2.0**0.5
f32 = jnp.float32
bf16 = jnp.bfloat16


def rings(axis_of_core):
    ids = np.arange(SIDE * SIDE * 4 * 2).reshape(SIDE, SIDE, 4, 2)
    out = []
    for x in range(4):
        for core in range(2):
            plane = ids[:, :, x, core]
            out += (plane if axis_of_core[core] == "y" else plane.T).tolist()
    return out


FIRST, SECOND = rings("yz"), rings("zy")


def sent_to_group(shard, groups):
    copies = jnp.broadcast_to(shard, (SIDE, *shard.shape))
    return lax.all_to_all(copies, ALL, 0, 0, axis_index_groups=groups, tiled=True)


def pairs(groups, by):
    return [(group[i], group[(i + by) % SIDE]) for group in groups for i in range(SIDE)]


def start_whole(place_ref, block, out, sem):
    rows = block.shape[0]
    at = pl.multiple_of(place_ref[0] * rows, rows)
    copy = pltpu.make_async_copy(block, out.at[pl.ds(at, rows)], sem)
    copy.start()
    copy.wait()


def whole_with(block, place):
    rows, columns = block.shape
    size = rows * columns
    return pl.pallas_call(
        start_whole,
        out_shape=jax.ShapeDtypeStruct((SIDE * rows, columns), block.dtype),
        in_specs=[pl.BlockSpec(memory_space=pltpu.SMEM), pl.BlockSpec(memory_space=pl.ANY)],
        out_specs=pl.BlockSpec(memory_space=pl.ANY),
        scratch_shapes=[pltpu.SemaphoreType.DMA],
        cost_estimate=pl.CostEstimate(flops=size, bytes_accessed=4 * size, transcendentals=0),
        compiler_params=pltpu.CompilerParams(vmem_limit_bytes=1 << 20),
        name="start_whole",
    )(place.astype(jnp.int32).reshape(1), block)


def ring_gathered(block, place):
    rows = block.shape[0]
    half = rows // 2
    whole = whole_with(block, place)

    def put(whole, piece, distance, row=0):
        at = lax.rem(place + distance, SIDE) * rows + row
        return lax.dynamic_update_slice_in_dim(whole, piece, at, 0)

    above = below = block
    for step in range(1, 4):
        above = lax.ppermute(above, ALL, pairs(SECOND, -1))
        below = lax.ppermute(below, ALL, pairs(SECOND, 1))
        whole = put(put(whole, above, step), below, SIDE - step)
    low = lax.ppermute(above[:half], ALL, pairs(SECOND, -1))
    high = lax.ppermute(below[half:], ALL, pairs(SECOND, 1))
    return put(put(whole, low, 4), high, 4, half)


def along_x(a, by):
    return lax.ppermute(a, "x", [(i, (i + by) % 4) for i in range(4)])


def partner_of(a):
    return lax.ppermute(a, "core", [(0, 1), (1, 0)])


def turned(core, a):
    return jnp.where(core == 0, a, jnp.swapaxes(a, 0, 1))


def all_ranks(shard, core):
    copies = jnp.broadcast_to(shard, (4, *shard.shape))
    mine = lax.all_to_all(copies, "x", 0, 0, tiled=True)
    other = partner_of(mine)
    both = jnp.stack([jnp.where(core == 0, mine, other), jnp.where(core == 0, other, mine)], 1)
    return both.reshape(SIDE, *shard.shape)


def joined_columns(parts):
    return jnp.moveaxis(parts, 0, 1).reshape(parts.shape[1], -1)


def causal_filter(gated, kernel):
    sequences = gated.shape[0] // LENGTH
    frames = gated.astype(f32).reshape(sequences, LENGTH, gated.shape[1])
    padded = jnp.pad(frames, ((0, 0), (KERNEL - 1, 0), (0, 0)))
    accumulated = jnp.zeros(frames.shape, f32)
    for offset in range(KERNEL):
        accumulated = (
            accumulated + kernel[offset].astype(f32) * padded[:, offset : offset + LENGTH]
        )
    return accumulated.reshape(gated.shape[0], gated.shape[1])


def row_norm_terms(values, entries):
    average = jnp.sum(values, 1, keepdims=True) / entries
    spread = jnp.maximum(jnp.sum(values * values, 1, keepdims=True) / entries - average * average, 0.0)
    return average, lax.rsqrt(spread + norm_eps)


def layer(
    tokens, w_value, w_gate, conv_kernel, conv_gain, w_mix_out, mix_gain, w_up, w_down, out_gain
):
    tp_rank = lax.axis_index(TP)
    core = lax.axis_index("core")
    frames = tokens.shape[0]
    width_part = tokens.shape[1]
    channel_part = w_value.shape[1]
    units_part = w_up.shape[1]

    def mine_of(vector, size):
        return lax.dynamic_slice_in_dim(vector, tp_rank * size, size, vector.ndim - 1)

    own_mix_gain = mine_of(mix_gain, width_part)
    own_out_gain = mine_of(out_gain, width_part)
    own_xt = tokens.T
    mix_rows = w_mix_out.shape[0]
    halves = [w_mix_out[:, :channel_part], w_mix_out[:, channel_part:]]
    shard = jnp.concatenate([w_up, w_down.T, w_value, w_gate, jnp.concatenate(halves, 0)], 1)
    shard = sent_to_group(shard, FIRST).reshape(-1, shard.shape[1])
    at = 2 * units_part
    wide = ring_gathered(shard[:, :at], jnp.where(core == 0, lax.axis_index("z"), lax.axis_index("y")))
    small = sent_to_group(shard[:, at:], SECOND)
    value_gate = small[:, :, : 2 * channel_part].reshape(WIDTH, 2 * channel_part)
    mix = small[:, :, 2 * channel_part :].reshape(SIDE, SIDE, 2, mix_rows, channel_part)
    mix = turned(core, mix.transpose(0, 1, 3, 2, 4)).reshape(CHANNELS, width_part)

    x_rank = lax.axis_index("x")
    mine = [own_xt, along_x(own_xt, -1), along_x(own_xt, 2), along_x(own_xt, 1)]
    mine = jnp.stack(mine)
    other = partner_of(mine)
    mine, other = jnp.roll(mine, x_rank, 0), jnp.roll(other, x_rank, 0)
    ranks = jnp.stack([jnp.where(core == 0, mine, other), jnp.where(core == 0, other, mine)], 1)
    ranks = turned(core, ranks.reshape(SIDE, SIDE, -1, frames)).reshape(WIDTH, frames)

    both = lax.dot_general(ranks, value_gate, (((0,), (0,)), ((), ())), preferred_element_type=f32)
    values_proj, gate_proj = both[:, :channel_part], both[:, channel_part:]
    gated = (values_proj * jax.nn.sigmoid(gate_proj)).astype(bf16)
    filtered = causal_filter(gated, mine_of(conv_kernel, channel_part))
    filtered_whole = joined_columns(all_ranks(filtered.astype(bf16), core)).astype(f32)
    average, scale = row_norm_terms(filtered_whole, CHANNELS)
    activated = jax.nn.silu((filtered_whole - average) * scale * conv_gain).astype(bf16)

    mixed = jnp.dot(activated, mix, preferred_element_type=f32)
    combined = residual_scale * tokens.astype(f32) + mixed
    combined_whole = all_ranks(combined.astype(bf16).T, core).reshape(WIDTH, frames).astype(f32)
    average = jnp.sum(combined_whole, 0) / WIDTH
    spread = jnp.maximum(jnp.sum(combined_whole * combined_whole, 0) / WIDTH - average * average, 0.0)
    scale = lax.rsqrt(spread + norm_eps)
    middle_whole = ((combined_whole - average) * scale * mix_gain[:, None]).astype(bf16)
    middle_whole = turned(core, middle_whole.reshape(SIDE, SIDE, -1, frames)).reshape(WIDTH, frames)
    middle = ((combined - average[:, None]) * scale[:, None] * own_mix_gain).astype(bf16)

    up_proj = lax.dot_general(
        wide[:, :units_part], middle_whole, (((0,), (0,)), ((), ())), preferred_element_type=f32
    )
    hidden = jnp.square(jax.nn.relu(up_proj)).astype(bf16)
    terms = jnp.dot(wide[:, units_part:], hidden, preferred_element_type=f32)
    terms = turned(core, terms.astype(bf16).reshape(SIDE, SIDE, -1, frames))
    terms = terms.reshape(4, 2, width_part, frames)
    kept = lax.dynamic_index_in_dim(terms, core, 1, keepdims=False)
    given = lax.dynamic_index_in_dim(terms, 1 - core, 1, keepdims=False)
    pair = (kept.astype(f32) + partner_of(given).astype(f32)).astype(bf16)
    arrived = lax.all_to_all(pair, "x", 0, 0, tiled=True)
    down_sum = jnp.sum(arrived.astype(f32), 0).T

    final = residual_scale * middle.astype(f32) + down_sum
    sums = jnp.stack([jnp.sum(final, 1), jnp.sum(final * final, 1)])
    copies = jnp.broadcast_to(sums, (SIDE, *sums.shape))
    totals = jnp.sum(lax.all_to_all(copies, TP, 0, 0, tiled=True), 0)
    average = totals[0] / WIDTH
    spread = jnp.maximum(totals[1] / WIDTH - average * average, 0.0)
    scale = lax.rsqrt(spread + norm_eps)
    result = (final - average[:, None]) * scale[:, None] * own_out_gain
    return result.astype(bf16)


def solution(mesh):
    split = Mesh(mesh.devices.reshape(8, 8, 4, 2), ALL)
    in_specs = (
        P(FS, TP),
        P(FS, TP),
        P(FS, TP),
        P(),
        P(),
        P(FS, TP),
        P(),
        P(FS, TP),
        P(TP, FS),
        P(),
    )
    return jax.shard_map(layer, mesh=split, in_specs=in_specs, out_specs=P(FS, TP), check_vma=False)
```

```python
import jax
import jax.numpy as jnp
import numpy as np
from jax import lax
from jax.sharding import Mesh
from jax.sharding import PartitionSpec as P


WIDTH = 2048
CHANNELS = 1024
KERNEL = 31
LENGTH = 128
FS = ("z", "y")
TP = ("x", "core")
ALL = ("z", "y", "x", "core")
SIDE = 8


norm_eps = 1e-05
residual_scale = 2.0**0.5
f32 = jnp.float32
bf16 = jnp.bfloat16


def rings(axis_of_core):
    ids = np.arange(SIDE * SIDE * 4 * 2).reshape(SIDE, SIDE, 4, 2)
    out = []
    for x in range(4):
        for core in range(2):
            plane = ids[:, :, x, core]
            out += (plane if axis_of_core[core] == "y" else plane.T).tolist()
    return out


FIRST, SECOND = rings("yz"), rings("zy")


def sent_to_group(shard, groups):
    copies = jnp.broadcast_to(shard, (SIDE, *shard.shape))
    return lax.all_to_all(copies, ALL, 0, 0, axis_index_groups=groups, tiled=True)


def along_x(a, by):
    return lax.ppermute(a, "x", [(i, (i + by) % 4) for i in range(4)])


def partner_of(a):
    return lax.ppermute(a, "core", [(0, 1), (1, 0)])


def turned(core, a):
    return jnp.where(core == 0, a, jnp.swapaxes(a, 0, 1))


def all_ranks(shard, core):
    copies = jnp.broadcast_to(shard, (4, *shard.shape))
    mine = lax.all_to_all(copies, "x", 0, 0, tiled=True)
    other = partner_of(mine)
    both = jnp.stack([jnp.where(core == 0, mine, other), jnp.where(core == 0, other, mine)], 1)
    return both.reshape(SIDE, *shard.shape)


def joined_columns(parts):
    return jnp.moveaxis(parts, 0, 1).reshape(parts.shape[1], -1)


def causal_filter(gated, kernel):
    sequences = gated.shape[0] // LENGTH
    frames = gated.astype(f32).reshape(sequences, LENGTH, gated.shape[1])
    padded = jnp.pad(frames, ((0, 0), (KERNEL - 1, 0), (0, 0)))
    accumulated = jnp.zeros(frames.shape, f32)
    for offset in range(KERNEL):
        accumulated = (
            accumulated + kernel[offset].astype(f32) * padded[:, offset : offset + LENGTH]
        )
    return accumulated.reshape(gated.shape[0], gated.shape[1])


def row_norm_terms(values, entries):
    average = jnp.sum(values, 1, keepdims=True) / entries
    spread = jnp.maximum(jnp.sum(values * values, 1, keepdims=True) / entries - average * average, 0.0)
    return average, lax.rsqrt(spread + norm_eps)


def layer(
    tokens, w_value, w_gate, conv_kernel, conv_gain, w_mix_out, mix_gain, w_up, w_down, out_gain
):
    tp_rank = lax.axis_index(TP)
    core = lax.axis_index("core")
    frames = tokens.shape[0]
    width_part = tokens.shape[1]
    channel_part = w_value.shape[1]
    units_part = w_up.shape[1]

    def mine_of(vector, size):
        return lax.dynamic_slice_in_dim(vector, tp_rank * size, size, vector.ndim - 1)

    wide = jnp.concatenate([w_up, w_down.T], 1)
    wide = lax.all_gather(wide, ALL, axis=0, tiled=True, axis_index_groups=FIRST)
    wide = lax.all_gather(wide, ALL, axis=0, tiled=True, axis_index_groups=SECOND)

    mix_rows = w_mix_out.shape[0]
    halves = [w_mix_out[:, :channel_part], w_mix_out[:, channel_part:]]
    small = jnp.concatenate([w_value, w_gate, jnp.concatenate(halves, 0)], 1)
    small = sent_to_group(small, FIRST).reshape(-1, small.shape[1])
    small = sent_to_group(small, SECOND)
    value_gate = small[:, :, : 2 * channel_part].reshape(WIDTH, 2 * channel_part)
    mix = small[:, :, 2 * channel_part :].reshape(SIDE, SIDE, 2, mix_rows, channel_part)
    mix = turned(core, mix.transpose(0, 1, 3, 2, 4)).reshape(CHANNELS, width_part)

    x_rank = lax.axis_index("x")
    own_mix_gain = mine_of(mix_gain, width_part)
    own_out_gain = mine_of(out_gain, width_part)
    own_xt = tokens.T
    parts = [own_xt, along_x(own_xt, -1), along_x(own_xt, 2), along_x(own_xt, 1)]
    mine = jnp.stack(parts)
    other = partner_of(mine)
    mine, other = jnp.roll(mine, x_rank, 0), jnp.roll(other, x_rank, 0)
    ranks = jnp.stack([jnp.where(core == 0, mine, other), jnp.where(core == 0, other, mine)], 1)
    ranks = turned(core, ranks.reshape(SIDE, SIDE, -1, frames)).reshape(WIDTH, frames)

    both = lax.dot_general(ranks, value_gate, (((0,), (0,)), ((), ())), preferred_element_type=f32)
    values_proj, gate_proj = both[:, :channel_part], both[:, channel_part:]
    gated = (values_proj * jax.nn.sigmoid(gate_proj)).astype(bf16)
    filtered = causal_filter(gated, mine_of(conv_kernel, channel_part))
    filtered_whole = joined_columns(all_ranks(filtered.astype(bf16), core)).astype(f32)
    average, scale = row_norm_terms(filtered_whole, CHANNELS)
    activated = jax.nn.silu((filtered_whole - average) * scale * conv_gain).astype(bf16)

    mixed = jnp.dot(activated, mix, preferred_element_type=f32)
    combined = residual_scale * tokens.astype(f32) + mixed
    combined_whole = all_ranks(combined.astype(bf16).T, core).reshape(WIDTH, frames).astype(f32)
    average = jnp.sum(combined_whole, 0) / WIDTH
    spread = jnp.maximum(jnp.sum(combined_whole * combined_whole, 0) / WIDTH - average * average, 0.0)
    scale = lax.rsqrt(spread + norm_eps)
    middle_whole = ((combined_whole - average) * scale * mix_gain[:, None]).astype(bf16)
    middle_whole = turned(core, middle_whole.reshape(SIDE, SIDE, -1, frames)).reshape(WIDTH, frames)
    middle = ((combined - average[:, None]) * scale[:, None] * own_mix_gain).astype(bf16)

    up_proj = lax.dot_general(
        wide[:, :units_part], middle_whole, (((0,), (0,)), ((), ())), preferred_element_type=f32
    )
    hidden = jnp.square(jax.nn.relu(up_proj)).astype(bf16)
    terms = jnp.dot(wide[:, units_part:], hidden, preferred_element_type=f32)
    terms = turned(core, terms.astype(bf16).reshape(SIDE, SIDE, -1, frames))
    terms = terms.reshape(4, 2, width_part, frames)
    kept = lax.dynamic_index_in_dim(terms, core, 1, keepdims=False)
    given = lax.dynamic_index_in_dim(terms, 1 - core, 1, keepdims=False)
    pair = (kept.astype(f32) + partner_of(given).astype(f32)).astype(bf16)
    arrived = lax.all_to_all(pair, "x", 0, 0, tiled=True)
    down_sum = jnp.sum(arrived.astype(f32), 0).T

    final = residual_scale * middle.astype(f32) + down_sum
    sums = jnp.stack([jnp.sum(final, 1), jnp.sum(final * final, 1)])
    copies = jnp.broadcast_to(sums, (SIDE, *sums.shape))
    totals = jnp.sum(lax.all_to_all(copies, TP, 0, 0, tiled=True), 0)
    average = totals[0] / WIDTH
    spread = jnp.maximum(totals[1] / WIDTH - average * average, 0.0)
    scale = lax.rsqrt(spread + norm_eps)
    result = (final - average[:, None]) * scale[:, None] * own_out_gain
    return result.astype(bf16)


def solution(mesh):
    split = Mesh(mesh.devices.reshape(8, 8, 4, 2), ALL)
    in_specs = (
        P(FS, TP),
        P(FS, TP),
        P(FS, TP),
        P(),
        P(),
        P(FS, TP),
        P(),
        P(FS, TP),
        P(TP, FS),
        P(),
    )
    return jax.shard_map(layer, mesh=split, in_specs=in_specs, out_specs=P(FS, TP), check_vma=False)
```

```python
import jax
import jax.numpy as jnp
import numpy as np
from jax import lax
from jax.sharding import Mesh
from jax.sharding import PartitionSpec as P


WIDTH = 2048
CHANNELS = 1024
KERNEL = 31
LENGTH = 128
FS = ("z", "y")
TP = ("x", "core")
ALL = ("z", "y", "x", "core")
SIDE = 8


norm_eps = 1e-05
residual_scale = 2.0**0.5
f32 = jnp.float32
bf16 = jnp.bfloat16


def rings(axis_of_core):
    ids = np.arange(SIDE * SIDE * 4 * 2).reshape(SIDE, SIDE, 4, 2)
    out = []
    for x in range(4):
        for core in range(2):
            plane = ids[:, :, x, core]
            out += (plane if axis_of_core[core] == "y" else plane.T).tolist()
    return out


FIRST, SECOND = rings("yz"), rings("zy")


def exchanged(copies, groups):
    return lax.all_to_all(copies, ALL, 0, 0, axis_index_groups=groups, tiled=True)


def sent_to_group(shard, groups):
    return exchanged(jnp.broadcast_to(shard, (SIDE, *shard.shape)), groups)


def along_x(a, by):
    return lax.ppermute(a, "x", [(i, (i + by) % 4) for i in range(4)])


def partner_of(a):
    return lax.ppermute(a, "core", [(0, 1), (1, 0)])


def turned(core, a):
    return jnp.where(core == 0, a, jnp.swapaxes(a, 0, 1))


def all_ranks(shard, core):
    copies = jnp.broadcast_to(shard, (4, *shard.shape))
    mine = lax.all_to_all(copies, "x", 0, 0, tiled=True)
    other = partner_of(mine)
    both = jnp.stack([jnp.where(core == 0, mine, other), jnp.where(core == 0, other, mine)], 1)
    return both.reshape(SIDE, *shard.shape)


def joined_columns(parts):
    return jnp.moveaxis(parts, 0, 1).reshape(parts.shape[1], -1)


def causal_filter(gated, kernel):
    sequences = gated.shape[0] // LENGTH
    frames = gated.astype(f32).reshape(sequences, LENGTH, gated.shape[1])
    padded = jnp.pad(frames, ((0, 0), (KERNEL - 1, 0), (0, 0)))
    accumulated = jnp.zeros(frames.shape, f32)
    for offset in range(KERNEL):
        accumulated = (
            accumulated + kernel[offset].astype(f32) * padded[:, offset : offset + LENGTH]
        )
    return accumulated.reshape(gated.shape[0], gated.shape[1])


def row_norm_terms(values, entries):
    average = jnp.sum(values, 1, keepdims=True) / entries
    spread = jnp.maximum(jnp.sum(values * values, 1, keepdims=True) / entries - average * average, 0.0)
    return average, lax.rsqrt(spread + norm_eps)


def layer(
    tokens, w_value, w_gate, conv_kernel, conv_gain, w_mix_out, mix_gain, w_up, w_down, out_gain
):
    tp_rank = lax.axis_index(TP)
    core = lax.axis_index("core")
    frames = tokens.shape[0]
    width_part = tokens.shape[1]
    channel_part = w_value.shape[1]
    units_part = w_up.shape[1]

    def mine_of(vector, size):
        return lax.dynamic_slice_in_dim(vector, tp_rank * size, size, vector.ndim - 1)

    own_mix_gain = mine_of(mix_gain, width_part)
    own_out_gain = mine_of(out_gain, width_part)
    own_xt = tokens.T
    mix_rows = w_mix_out.shape[0]
    halves = [w_mix_out[:, :channel_part], w_mix_out[:, channel_part:]]
    wide = jnp.concatenate([w_up, w_down.T], 1)
    small = jnp.concatenate([w_value, w_gate, jnp.concatenate(halves, 0)], 1)
    wide, small = lax.optimization_barrier((wide, small))
    copies = [jnp.broadcast_to(a, (SIDE, *a.shape)) for a in (wide, small)]
    shard = exchanged(jnp.concatenate(copies, 2), FIRST)
    shard = shard.reshape(-1, shard.shape[2])
    at = 2 * units_part
    wide = lax.all_gather(shard[:, :at], ALL, axis=0, tiled=True, axis_index_groups=SECOND)
    small = sent_to_group(shard[:, at:], SECOND)
    value_gate = small[:, :, : 2 * channel_part].reshape(WIDTH, 2 * channel_part)
    mix = small[:, :, 2 * channel_part :].reshape(SIDE, SIDE, 2, mix_rows, channel_part)
    mix = turned(core, mix.transpose(0, 1, 3, 2, 4)).reshape(CHANNELS, width_part)

    x_rank = lax.axis_index("x")
    mine = [own_xt, along_x(own_xt, -1), along_x(own_xt, 2), along_x(own_xt, 1)]
    mine = jnp.stack(mine)
    other = partner_of(mine)
    mine, other = jnp.roll(mine, x_rank, 0), jnp.roll(other, x_rank, 0)
    ranks = jnp.stack([jnp.where(core == 0, mine, other), jnp.where(core == 0, other, mine)], 1)
    ranks = turned(core, ranks.reshape(SIDE, SIDE, -1, frames)).reshape(WIDTH, frames)

    both = lax.dot_general(ranks, value_gate, (((0,), (0,)), ((), ())), preferred_element_type=f32)
    values_proj, gate_proj = both[:, :channel_part], both[:, channel_part:]
    gated = (values_proj * jax.nn.sigmoid(gate_proj)).astype(bf16)
    filtered = causal_filter(gated, mine_of(conv_kernel, channel_part))
    filtered_whole = joined_columns(all_ranks(filtered.astype(bf16), core)).astype(f32)
    average, scale = row_norm_terms(filtered_whole, CHANNELS)
    activated = jax.nn.silu((filtered_whole - average) * scale * conv_gain).astype(bf16)

    mixed = jnp.dot(activated, mix, preferred_element_type=f32)
    combined = residual_scale * tokens.astype(f32) + mixed
    combined_whole = all_ranks(combined.astype(bf16).T, core).reshape(WIDTH, frames).astype(f32)
    average = jnp.sum(combined_whole, 0) / WIDTH
    spread = jnp.maximum(jnp.sum(combined_whole * combined_whole, 0) / WIDTH - average * average, 0.0)
    scale = lax.rsqrt(spread + norm_eps)
    middle_whole = ((combined_whole - average) * scale * mix_gain[:, None]).astype(bf16)
    middle_whole = turned(core, middle_whole.reshape(SIDE, SIDE, -1, frames)).reshape(WIDTH, frames)
    middle = ((combined - average[:, None]) * scale[:, None] * own_mix_gain).astype(bf16)

    up_proj = lax.dot_general(
        wide[:, :units_part], middle_whole, (((0,), (0,)), ((), ())), preferred_element_type=f32
    )
    hidden = jnp.square(jax.nn.relu(up_proj)).astype(bf16)
    terms = jnp.dot(wide[:, units_part:], hidden, preferred_element_type=f32)
    terms = turned(core, terms.astype(bf16).reshape(SIDE, SIDE, -1, frames))
    terms = terms.reshape(4, 2, width_part, frames)
    kept = lax.dynamic_index_in_dim(terms, core, 1, keepdims=False)
    given = lax.dynamic_index_in_dim(terms, 1 - core, 1, keepdims=False)
    pair = (kept.astype(f32) + partner_of(given).astype(f32)).astype(bf16)
    arrived = lax.all_to_all(pair, "x", 0, 0, tiled=True)
    down_sum = jnp.sum(arrived.astype(f32), 0).T

    final = residual_scale * middle.astype(f32) + down_sum
    sums = jnp.stack([jnp.sum(final, 1), jnp.sum(final * final, 1)])
    copies = jnp.broadcast_to(sums, (SIDE, *sums.shape))
    totals = jnp.sum(lax.all_to_all(copies, TP, 0, 0, tiled=True), 0)
    average = totals[0] / WIDTH
    spread = jnp.maximum(totals[1] / WIDTH - average * average, 0.0)
    scale = lax.rsqrt(spread + norm_eps)
    result = (final - average[:, None]) * scale[:, None] * own_out_gain
    return result.astype(bf16)


def solution(mesh):
    split = Mesh(mesh.devices.reshape(8, 8, 4, 2), ALL)
    in_specs = (
        P(FS, TP),
        P(FS, TP),
        P(FS, TP),
        P(),
        P(),
        P(FS, TP),
        P(),
        P(FS, TP),
        P(TP, FS),
        P(),
    )
    return jax.shard_map(layer, mesh=split, in_specs=in_specs, out_specs=P(FS, TP), check_vma=False)
```

```python
import jax
import jax.numpy as jnp
import numpy as np
from jax import lax
from jax.sharding import Mesh
from jax.sharding import PartitionSpec as P


WIDTH = 2048
CHANNELS = 1024
KERNEL = 31
LENGTH = 128
FS = ("z", "y")
TP = ("x", "core")
ALL = ("z", "y", "x", "core")
SIDE = 8


norm_eps = 1e-05
residual_scale = 2.0**0.5
f32 = jnp.float32
bf16 = jnp.bfloat16


def rings(axis_of_core):
    ids = np.arange(SIDE * SIDE * 4 * 2).reshape(SIDE, SIDE, 4, 2)
    out = []
    for x in range(4):
        for core in range(2):
            plane = ids[:, :, x, core]
            out += (plane if axis_of_core[core] == "y" else plane.T).tolist()
    return out


FIRST, SECOND = rings("yz"), rings("zy")


def exchanged(copies, groups):
    return lax.all_to_all(copies, ALL, 0, 0, axis_index_groups=groups, tiled=True)


def sent_to_group(shard, groups):
    return exchanged(jnp.broadcast_to(shard, (SIDE, *shard.shape)), groups)


def along_x(a, by):
    return lax.ppermute(a, "x", [(i, (i + by) % 4) for i in range(4)])


def partner_of(a):
    return lax.ppermute(a, "core", [(0, 1), (1, 0)])


def turned(core, a):
    return jnp.where(core == 0, a, jnp.swapaxes(a, 0, 1))


def all_ranks(shard, core):
    copies = jnp.broadcast_to(shard, (4, *shard.shape))
    mine = lax.all_to_all(copies, "x", 0, 0, tiled=True)
    other = partner_of(mine)
    both = jnp.stack([jnp.where(core == 0, mine, other), jnp.where(core == 0, other, mine)], 1)
    return both.reshape(SIDE, *shard.shape)


def joined_columns(parts):
    return jnp.moveaxis(parts, 0, 1).reshape(parts.shape[1], -1)


def causal_filter(gated, kernel):
    sequences = gated.shape[0] // LENGTH
    frames = gated.astype(f32).reshape(sequences, LENGTH, gated.shape[1])
    padded = jnp.pad(frames, ((0, 0), (KERNEL - 1, 0), (0, 0)))
    accumulated = jnp.zeros(frames.shape, f32)
    for offset in range(KERNEL):
        accumulated = (
            accumulated + kernel[offset].astype(f32) * padded[:, offset : offset + LENGTH]
        )
    return accumulated.reshape(gated.shape[0], gated.shape[1])


def row_norm_terms(values, entries):
    average = jnp.sum(values, 1, keepdims=True) / entries
    spread = jnp.maximum(jnp.sum(values * values, 1, keepdims=True) / entries - average * average, 0.0)
    return average, lax.rsqrt(spread + norm_eps)


def layer(
    tokens, w_value, w_gate, conv_kernel, conv_gain, w_mix_out, mix_gain, w_up, w_down, out_gain
):
    tp_rank = lax.axis_index(TP)
    core = lax.axis_index("core")
    frames = tokens.shape[0]
    width_part = tokens.shape[1]
    channel_part = w_value.shape[1]
    units_part = w_up.shape[1]

    def mine_of(vector, size):
        return lax.dynamic_slice_in_dim(vector, tp_rank * size, size, vector.ndim - 1)

    own_mix_gain = mine_of(mix_gain, width_part)
    own_out_gain = mine_of(out_gain, width_part)
    own_xt = tokens.T
    mix_rows = w_mix_out.shape[0]
    halves = [w_mix_out[:, :channel_part], w_mix_out[:, channel_part:]]
    wide = jnp.concatenate([w_up, w_down.T, w_value, w_gate], 1)
    wide, small = lax.optimization_barrier((wide, jnp.concatenate(halves, 0)))
    copies = [jnp.broadcast_to(a, (SIDE, *a.shape)) for a in (wide, small)]
    shard = exchanged(jnp.concatenate(copies, 2), FIRST)
    shard = shard.reshape(-1, shard.shape[2])
    at = 2 * units_part
    wide = shard[:, :at]
    wide = lax.all_gather(wide, ALL, axis=0, tiled=True, axis_index_groups=SECOND)
    small = sent_to_group(shard[:, at:], SECOND)
    value_gate = small[:, :, : 2 * channel_part].reshape(WIDTH, 2 * channel_part)
    mix = small[:, :, 2 * channel_part :].reshape(SIDE, SIDE, 2, mix_rows, channel_part)
    mix = turned(core, mix.transpose(0, 1, 3, 2, 4)).reshape(CHANNELS, width_part)

    x_rank = lax.axis_index("x")
    mine = [own_xt, along_x(own_xt, -1), along_x(own_xt, 2), along_x(own_xt, 1)]
    mine = jnp.stack(mine)
    other = partner_of(mine)
    mine, other = jnp.roll(mine, x_rank, 0), jnp.roll(other, x_rank, 0)
    ranks = jnp.stack([jnp.where(core == 0, mine, other), jnp.where(core == 0, other, mine)], 1)
    ranks = turned(core, ranks.reshape(SIDE, SIDE, -1, frames)).reshape(WIDTH, frames)
    shift = residual_scale * jnp.mean(ranks.astype(f32), 0)

    both = lax.dot_general(ranks, value_gate, (((0,), (0,)), ((), ())), preferred_element_type=f32)
    values_proj, gate_proj = both[:, :channel_part], both[:, channel_part:]
    gated = (values_proj * jax.nn.sigmoid(gate_proj)).astype(bf16)
    filtered = causal_filter(gated, mine_of(conv_kernel, channel_part))
    filtered_whole = joined_columns(all_ranks(filtered.astype(bf16), core)).astype(f32)
    average, scale = row_norm_terms(filtered_whole, CHANNELS)
    activated = jax.nn.silu((filtered_whole - average) * scale * conv_gain).astype(bf16)

    mixed = jnp.dot(activated, mix, preferred_element_type=f32)
    combined = residual_scale * tokens.astype(f32) + mixed - shift[:, None]
    combined_whole = all_ranks(combined.astype(bf16).T, core).reshape(WIDTH, frames).astype(f32)
    average = jnp.sum(combined_whole, 0) / WIDTH
    spread = jnp.maximum(jnp.sum(combined_whole * combined_whole, 0) / WIDTH - average * average, 0.0)
    scale = lax.rsqrt(spread + norm_eps)
    middle_whole = ((combined_whole - average) * scale * mix_gain[:, None]).astype(bf16)
    middle_whole = turned(core, middle_whole.reshape(SIDE, SIDE, -1, frames)).reshape(WIDTH, frames)
    middle = ((combined - average[:, None]) * scale[:, None] * own_mix_gain).astype(bf16)

    up_proj = lax.dot_general(
        wide[:, :units_part], middle_whole, (((0,), (0,)), ((), ())), preferred_element_type=f32
    )
    hidden = jnp.square(jax.nn.relu(up_proj)).astype(bf16)
    terms = jnp.dot(wide[:, units_part:], hidden, preferred_element_type=f32)
    terms = turned(core, terms.astype(bf16).reshape(SIDE, SIDE, -1, frames))
    terms = terms.reshape(4, 2, width_part, frames)
    kept = lax.dynamic_index_in_dim(terms, core, 1, keepdims=False)
    given = lax.dynamic_index_in_dim(terms, 1 - core, 1, keepdims=False)
    pair = (kept.astype(f32) + partner_of(given).astype(f32)).astype(bf16)
    arrived = lax.all_to_all(pair, "x", 0, 0, tiled=True)
    down_sum = jnp.sum(arrived.astype(f32), 0).T

    final = residual_scale * middle.astype(f32) + down_sum
    sums = jnp.stack([jnp.sum(final, 1), jnp.sum(final * final, 1)])
    copies = jnp.broadcast_to(sums, (SIDE, *sums.shape))
    totals = jnp.sum(lax.all_to_all(copies, TP, 0, 0, tiled=True), 0)
    average = totals[0] / WIDTH
    spread = jnp.maximum(totals[1] / WIDTH - average * average, 0.0)
    scale = lax.rsqrt(spread + norm_eps)
    result = (final - average[:, None]) * scale[:, None] * own_out_gain
    return result.astype(bf16)


def solution(mesh):
    split = Mesh(mesh.devices.reshape(8, 8, 4, 2), ALL)
    in_specs = (
        P(FS, TP),
        P(FS, TP),
        P(FS, TP),
        P(),
        P(),
        P(FS, TP),
        P(),
        P(FS, TP),
        P(TP, FS),
        P(),
    )
    return jax.shard_map(layer, mesh=split, in_specs=in_specs, out_specs=P(FS, TP), check_vma=False)
```

```python
import jax
import jax.numpy as jnp
import numpy as np
from jax import lax
from jax.sharding import Mesh
from jax.sharding import PartitionSpec as P


WIDTH = 2048
CHANNELS = 1024
KERNEL = 31
LENGTH = 128
FS = ("z", "y")
TP = ("x", "core")
ALL = ("z", "y", "x", "core")
SIDE = 8


norm_eps = 1e-05
residual_scale = 2.0**0.5
f32 = jnp.float32
bf16 = jnp.bfloat16


def rings(axis_of_core):
    ids = np.arange(SIDE * SIDE * 4 * 2).reshape(SIDE, SIDE, 4, 2)
    out = []
    for x in range(4):
        for core in range(2):
            plane = ids[:, :, x, core]
            out += (plane if axis_of_core[core] == "y" else plane.T).tolist()
    return out


FIRST, SECOND = rings("yz"), rings("zy")


def exchanged(copies, groups):
    return lax.all_to_all(copies, ALL, 0, 0, axis_index_groups=groups, tiled=True)


def sent_to_group(shard, groups):
    return exchanged(jnp.broadcast_to(shard, (SIDE, *shard.shape)), groups)


def along_x(a, by):
    return lax.ppermute(a, "x", [(i, (i + by) % 4) for i in range(4)])


def partner_of(a):
    return lax.ppermute(a, "core", [(0, 1), (1, 0)])


def turned(core, a):
    return jnp.where(core == 0, a, jnp.swapaxes(a, 0, 1))


def all_ranks(shard, core):
    copies = jnp.broadcast_to(shard, (4, *shard.shape))
    mine = lax.all_to_all(copies, "x", 0, 0, tiled=True)
    other = partner_of(mine)
    both = jnp.stack([jnp.where(core == 0, mine, other), jnp.where(core == 0, other, mine)], 1)
    return both.reshape(SIDE, *shard.shape)


def all_at_once(shard):
    copies = jnp.broadcast_to(shard, (SIDE, *shard.shape))
    return lax.all_to_all(copies, TP, 0, 0, tiled=True)


def joined_columns(parts):
    return jnp.moveaxis(parts, 0, 1).reshape(parts.shape[1], -1)


def causal_filter(gated, kernel):
    sequences = gated.shape[0] // LENGTH
    frames = gated.astype(f32).reshape(sequences, LENGTH, gated.shape[1])
    padded = jnp.pad(frames, ((0, 0), (KERNEL - 1, 0), (0, 0)))
    accumulated = jnp.zeros(frames.shape, f32)
    for offset in range(KERNEL):
        accumulated = (
            accumulated + kernel[offset].astype(f32) * padded[:, offset : offset + LENGTH]
        )
    return accumulated.reshape(gated.shape[0], gated.shape[1])


def row_norm_terms(values, entries):
    average = jnp.sum(values, 1, keepdims=True) / entries
    spread = jnp.maximum(jnp.sum(values * values, 1, keepdims=True) / entries - average * average, 0.0)
    return average, lax.rsqrt(spread + norm_eps)


def layer(
    tokens, w_value, w_gate, conv_kernel, conv_gain, w_mix_out, mix_gain, w_up, w_down, out_gain
):
    tp_rank = lax.axis_index(TP)
    core = lax.axis_index("core")
    frames = tokens.shape[0]
    width_part = tokens.shape[1]
    channel_part = w_value.shape[1]
    units_part = w_up.shape[1]

    def mine_of(vector, size):
        return lax.dynamic_slice_in_dim(vector, tp_rank * size, size, vector.ndim - 1)

    own_mix_gain = mine_of(mix_gain, width_part)
    own_out_gain = mine_of(out_gain, width_part)
    own_xt = tokens.T
    mix_rows = w_mix_out.shape[0]
    halves = [w_mix_out[:, :channel_part], w_mix_out[:, channel_part:]]
    wide = jnp.concatenate([w_up, w_down.T, w_value, w_gate], 1)
    wide, small = lax.optimization_barrier((wide, jnp.concatenate(halves, 0)))
    copies = [jnp.broadcast_to(a, (SIDE, *a.shape)) for a in (wide, small)]
    shard = exchanged(jnp.concatenate(copies, 2), FIRST)
    shard = shard.reshape(-1, shard.shape[2])
    at = 2 * units_part
    wide = shard[:, :at]
    wide = lax.all_gather(wide, ALL, axis=0, tiled=True, axis_index_groups=SECOND)
    small = sent_to_group(shard[:, at:], SECOND)
    value_gate = small[:, :, : 2 * channel_part].reshape(WIDTH, 2 * channel_part)
    mix = small[:, :, 2 * channel_part :].reshape(SIDE, SIDE, 2, mix_rows, channel_part)
    mix = turned(core, mix.transpose(0, 1, 3, 2, 4)).reshape(CHANNELS, width_part)

    x_rank = lax.axis_index("x")
    mine = [own_xt, along_x(own_xt, -1), along_x(own_xt, 2), along_x(own_xt, 1)]
    mine = jnp.stack(mine)
    other = partner_of(mine)
    mine, other = jnp.roll(mine, x_rank, 0), jnp.roll(other, x_rank, 0)
    ranks = jnp.stack([jnp.where(core == 0, mine, other), jnp.where(core == 0, other, mine)], 1)
    ranks = turned(core, ranks.reshape(SIDE, SIDE, -1, frames)).reshape(WIDTH, frames)
    shift = residual_scale * jnp.mean(ranks.astype(f32), 0)

    both = lax.dot_general(ranks, value_gate, (((0,), (0,)), ((), ())), preferred_element_type=f32)
    values_proj, gate_proj = both[:, :channel_part], both[:, channel_part:]
    gated = (values_proj * jax.nn.sigmoid(gate_proj)).astype(bf16)
    filtered = causal_filter(gated, mine_of(conv_kernel, channel_part))
    filtered_whole = joined_columns(all_at_once(filtered.astype(bf16))).astype(f32)
    average, scale = row_norm_terms(filtered_whole, CHANNELS)
    activated = jax.nn.silu((filtered_whole - average) * scale * conv_gain).astype(bf16)

    mixed = jnp.dot(activated, mix, preferred_element_type=f32)
    combined = residual_scale * tokens.astype(f32) + mixed - shift[:, None]
    combined_whole = all_ranks(combined.astype(bf16).T, core).reshape(WIDTH, frames).astype(f32)
    average = jnp.sum(combined_whole, 0) / WIDTH
    spread = jnp.maximum(jnp.sum(combined_whole * combined_whole, 0) / WIDTH - average * average, 0.0)
    scale = lax.rsqrt(spread + norm_eps)
    middle_whole = ((combined_whole - average) * scale * mix_gain[:, None]).astype(bf16)
    middle_whole = turned(core, middle_whole.reshape(SIDE, SIDE, -1, frames)).reshape(WIDTH, frames)
    middle = ((combined - average[:, None]) * scale[:, None] * own_mix_gain).astype(bf16)

    up_proj = lax.dot_general(
        wide[:, :units_part], middle_whole, (((0,), (0,)), ((), ())), preferred_element_type=f32
    )
    hidden = jnp.square(jax.nn.relu(up_proj)).astype(bf16)
    terms = jnp.dot(wide[:, units_part:], hidden, preferred_element_type=f32)
    terms = turned(core, terms.astype(bf16).reshape(SIDE, SIDE, -1, frames))
    terms = terms.reshape(4, 2, width_part, frames)
    kept = lax.dynamic_index_in_dim(terms, core, 1, keepdims=False)
    given = lax.dynamic_index_in_dim(terms, 1 - core, 1, keepdims=False)
    pair = (kept.astype(f32) + partner_of(given).astype(f32)).astype(bf16)
    arrived = lax.all_to_all(pair, "x", 0, 0, tiled=True)
    down_sum = jnp.sum(arrived.astype(f32), 0).T

    final = residual_scale * middle.astype(f32) + down_sum
    sums = jnp.stack([jnp.sum(final, 1), jnp.sum(final * final, 1)])
    copies = jnp.broadcast_to(sums, (SIDE, *sums.shape))
    totals = jnp.sum(lax.all_to_all(copies, TP, 0, 0, tiled=True), 0)
    average = totals[0] / WIDTH
    spread = jnp.maximum(totals[1] / WIDTH - average * average, 0.0)
    scale = lax.rsqrt(spread + norm_eps)
    result = (final - average[:, None]) * scale[:, None] * own_out_gain
    return result.astype(bf16)


def solution(mesh):
    split = Mesh(mesh.devices.reshape(8, 8, 4, 2), ALL)
    in_specs = (
        P(FS, TP),
        P(FS, TP),
        P(FS, TP),
        P(),
        P(),
        P(FS, TP),
        P(),
        P(FS, TP),
        P(TP, FS),
        P(),
    )
    return jax.shard_map(layer, mesh=split, in_specs=in_specs, out_specs=P(FS, TP), check_vma=False)
```
